256 devices in a mesh: grp: 2 (over y), fs: 16 (over z), tp: 8 (over x, core).
Axes of the slice: x: 4, y: 2, z: 16, core: 2. Of those that a mesh axis runs over, the one named last changes fastest.
The devices are a block of a 4x16x16 slice.
Arguments:
- stream: bfloat16 [2048, 12288], P('tp', ('grp', 'fs')), parts along dimension 1, may hold values from -6 to 6
- first_gain: float32 [2048], replicated, may hold values from 0.1 to 1.9
- first_gate: float32 [2048, 5632], P('fs', 'tp'), may hold values from -0.125 to 0.125
- first_gate_scale: float32 [5632], P('tp'), may hold values from 0.5 to 2
- first_up: float32 [2048, 5632], P('fs', 'tp'), may hold values from -0.125 to 0.125
- first_up_scale: float32 [5632], P('tp'), may hold values from 0.5 to 2
- first_down: float32 [5632, 2048], P('tp', 'fs'), may hold values from -0.078125 to 0.078125
- first_down_scale: float32 [2048], P('fs'), may hold values from 0.5 to 2
- mixer_gain: float32 [2048], replicated, may hold values from 0.1 to 1.9
- mixer_left: float32 [2048, 1024], P('fs', 'tp'), may hold values from -0.125 to 0.125
- mixer_left_scale: float32 [1024], P('tp'), may hold values from 0.5 to 2
- mixer_right: float32 [2048, 1024], P('fs', 'tp'), may hold values from -0.125 to 0.125
- mixer_right_scale: float32 [1024], P('tp'), may hold values from 0.5 to 2
- channel_gain: float32 [1024], P('tp'), may hold values from 0.1 to 1.9
- spatial: bfloat16 [8, 128, 128], P('tp'), may hold values from -0.5 to 0.5
- spatial_bias: float32 [8, 128], P('tp'), may hold values from 0.1 to 1.9
- mixer_out: float32 [1024, 2048], P('tp', 'fs'), may hold values from -0.1875 to 0.1875
- mixer_out_scale: float32 [2048], P('fs'), may hold values from 0.5 to 2
- second_gain: float32 [2048], replicated, may hold values from 0.1 to 1.9
- second_gate: float32 [2048, 5632], P('fs', 'tp'), may hold values from -0.125 to 0.125
- second_gate_scale: float32 [5632], P('tp'), may hold values from 0.5 to 2
- second_up: float32 [2048, 5632], P('fs', 'tp'), may hold values from -0.125 to 0.125
- second_up_scale: float32 [5632], P('tp'), may hold values from 0.5 to 2
- second_down: float32 [5632, 2048], P('tp', 'fs'), may hold values from -0.078125 to 0.078125
- second_down_scale: float32 [2048], P('fs'), may hold values from 0.5 to 2
Outputs:
- result: bfloat16 [2048, 12288], P('tp', ('grp', 'fs')), parts along dimension 1
The draws below stay inside these ranges and needn't reach their ends.
There are 2 independent parts, one for each index of `grp`. The reference program is written for one: setup_inputs(seed, part) draws one part's arguments, and reference() takes and returns one part's arrays. A program takes and returns all parts, laid end to end along the dimension named above; an argument that names none is the same for every part. Nothing has to cross between parts.
All inputs are finite; a program needn't handle non-finite values.
Results may differ from the reference program's by a relative error of at most 0.02.
Values may be sent and summed in bfloat16 or wider, within the bound.
No kernel may reach another device: no remote copies, remote signals or barrier semaphores. Data moves between devices by JAX's collectives and lax.ppermute only.
A program may use at most 128 MiB of HBM per device.

```python
import math
import jax
import jax.numpy as jnp
from jax import lax

D = 2048
FF = 5632
BRANCH = 1024
GROUPS = 8
BLOCK = 128
TOKENS = 6144
N_TP = 8


def steps_of(rng, dims, split, least, largest):
    def one(axis_at, shards_of):
        draws = jax.random.uniform(jax.random.fold_in(jax.random.fold_in(rng, 6), axis_at), (shards_of,), jnp.float32, least / len(split), largest / len(split))
        return jnp.repeat(jnp.exp(draws), dims[axis_at] // shards_of).reshape((-1,) + (1,) * (len(dims) - axis_at - 1))

    level = one(*split[0])
    for cut in split[1:]:
        level = level * one(*cut)
    return level


def normal_values(own_key, shape, scale, most, split=(), kind=jnp.bfloat16):
    values = jax.random.normal(own_key, shape, jnp.float32) * scale
    if len(split) > 0:
        values = steps_of(own_key, shape, split, -0.22, 0.18) * values
    return jnp.clip(values, min=-most, max=most).astype(kind)


def setup_inputs(seed: int = 0, part: int = 0) -> dict:
    key_of = jax.random.split(jax.random.key(seed), 26)
    own_keys = jax.random.split(jax.random.fold_in(key_of[25], part), 26)
    return {
        "stream": normal_values(own_keys[0], (D, TOKENS), 1.0, 6.0, ((0, 8), (1, 16))),
        "first_gain": jnp.clip(1.0 + 0.18 * jax.random.normal(key_of[1], (D,), jnp.float32), 0.1, 1.9),
        "first_gate": normal_values(key_of[2], (D, FF), D ** -0.5, 0.125, ((0, 16), (1, 8)), jnp.float32),
        "first_gate_scale": jnp.clip(jnp.exp(math.log(2.0) - 1.3862944 * jax.random.uniform(key_of[3], (FF,), jnp.float32) ** steps_of(key_of[3], (FF,), ((0, 8),), -0.2, 0.2)), 0.5, 2.0),
        "first_up": normal_values(key_of[4], (D, FF), D ** -0.5, 0.125, ((0, 16), (1, 8)), jnp.float32),
        "first_up_scale": jnp.clip(jnp.exp(math.log(2.0) - 1.3862944 * jax.random.uniform(key_of[5], (FF,), jnp.float32) ** steps_of(key_of[5], (FF,), ((0, 8),), -0.2, 0.2)), 0.5, 2.0),
        "first_down": normal_values(key_of[6], (FF, D), FF ** -0.5, 0.078125, ((0, 8), (1, 16)), jnp.float32),
        "first_down_scale": jnp.clip(jnp.exp(math.log(2.0) - 1.3862944 * jax.random.uniform(key_of[7], (D,), jnp.float32) ** steps_of(key_of[7], (D,), ((0, 16),), -0.2, 0.2)), 0.5, 2.0),
        "mixer_gain": jnp.clip(1.0 + 0.18 * jax.random.normal(key_of[8], (D,), jnp.float32), 0.1, 1.9),
        "mixer_left": normal_values(key_of[9], (D, BRANCH), D ** -0.5, 0.125, ((0, 16), (1, 8)), jnp.float32),
        "mixer_left_scale": jnp.clip(jnp.exp(math.log(2.0) - 1.3862944 * jax.random.uniform(key_of[10], (BRANCH,), jnp.float32) ** steps_of(key_of[10], (BRANCH,), ((0, 8),), -0.2, 0.2)), 0.5, 2.0),
        "mixer_right": normal_values(key_of[11], (D, BRANCH), D ** -0.5, 0.125, ((0, 16), (1, 8)), jnp.float32),
        "mixer_right_scale": jnp.clip(jnp.exp(math.log(2.0) - 1.3862944 * jax.random.uniform(key_of[12], (BRANCH,), jnp.float32) ** steps_of(key_of[12], (BRANCH,), ((0, 8),), -0.2, 0.2)), 0.5, 2.0),
        "channel_gain": jnp.clip(1.0 + 0.18 * jax.random.normal(key_of[13], (BRANCH,), jnp.float32), 0.1, 1.9),
        "spatial": normal_values(key_of[14], (GROUPS, BLOCK, BLOCK), BLOCK ** -0.5, 0.5, ((0, 8),)),
        "spatial_bias": jnp.clip(1.0 + 0.18 * jax.random.normal(key_of[15], (GROUPS, BLOCK), jnp.float32), 0.1, 1.9),
        "mixer_out": normal_values(key_of[16], (BRANCH, D), BRANCH ** -0.5, 0.1875, ((0, 8), (1, 16)), jnp.float32),
        "mixer_out_scale": jnp.clip(jnp.exp(math.log(2.0) - 1.3862944 * jax.random.uniform(key_of[17], (D,), jnp.float32) ** steps_of(key_of[17], (D,), ((0, 16),), -0.2, 0.2)), 0.5, 2.0),
        "second_gain": jnp.clip(1.0 + 0.18 * jax.random.normal(key_of[18], (D,), jnp.float32), 0.1, 1.9),
        "second_gate": normal_values(key_of[19], (D, FF), D ** -0.5, 0.125, ((0, 16), (1, 8)), jnp.float32),
        "second_gate_scale": jnp.clip(jnp.exp(math.log(2.0) - 1.3862944 * jax.random.uniform(key_of[20], (FF,), jnp.float32) ** steps_of(key_of[20], (FF,), ((0, 8),), -0.2, 0.2)), 0.5, 2.0),
        "second_up": normal_values(key_of[21], (D, FF), D ** -0.5, 0.125, ((0, 16), (1, 8)), jnp.float32),
        "second_up_scale": jnp.clip(jnp.exp(math.log(2.0) - 1.3862944 * jax.random.uniform(key_of[22], (FF,), jnp.float32) ** steps_of(key_of[22], (FF,), ((0, 8),), -0.2, 0.2)), 0.5, 2.0),
        "second_down": normal_values(key_of[23], (FF, D), FF ** -0.5, 0.078125, ((0, 8), (1, 16)), jnp.float32),
        "second_down_scale": jnp.clip(jnp.exp(math.log(2.0) - 1.3862944 * jax.random.uniform(key_of[24], (D,), jnp.float32) ** steps_of(key_of[24], (D,), ((0, 16),), -0.2, 0.2)), 0.5, 2.0),
    }


EPS = 1e-06

def rms_rows(stream, gain):
    values = stream.astype(jnp.float32)
    inverse = lax.rsqrt(lax.optimization_barrier(jnp.mean(values * values, axis=0)) + EPS)
    return (values * inverse * gain[:, None]).astype(jnp.bfloat16)

def project(weight, scale, inputs):
    product = lax.dot_general(weight.astype(jnp.bfloat16), inputs, (((0,), (0,)), ((), ())), preferred_element_type=jnp.float32)
    return product * scale[:, None]

def block_sum(weight, scale, hidden):
    width = weight.shape[0] // N_TP
    total = jnp.zeros((weight.shape[1], hidden.shape[1]), jnp.float32)
    for index in range(N_TP):
        term = project(weight[index * width:(index + 1) * width], scale, hidden[index * width:(index + 1) * width])
        total = total + lax.optimization_barrier(term.astype(jnp.bfloat16)).astype(jnp.float32)
    return total

def half_step(stream, gain, gate_weight, gate_scale, up_weight, up_scale, down_weight, down_scale):
    normed_rows = rms_rows(stream, gain)
    gate = project(gate_weight, gate_scale, normed_rows)
    upward = project(up_weight, up_scale, normed_rows)
    hidden = (jax.nn.silu(gate) * upward).astype(jnp.bfloat16)
    total = block_sum(down_weight, down_scale, hidden)
    return (stream.astype(jnp.float32) + 0.5 * total).astype(jnp.bfloat16)

def reference(stream, first_gain, first_gate, first_gate_scale, first_up, first_up_scale, first_down, first_down_scale, mixer_gain, mixer_left, mixer_left_scale, mixer_right, mixer_right_scale, channel_gain, spatial, spatial_bias, mixer_out, mixer_out_scale, second_gain, second_gate, second_gate_scale, second_up, second_up_scale, second_down, second_down_scale):
    stream = half_step(stream, first_gain, first_gate, first_gate_scale, first_up, first_up_scale, first_down, first_down_scale)
    normed_rows = rms_rows(stream, mixer_gain)
    left = jax.nn.gelu(project(mixer_left, mixer_left_scale, normed_rows))
    right = jax.nn.gelu(project(mixer_right, mixer_right_scale, normed_rows))
    average = lax.optimization_barrier(jnp.mean(right, axis=0))
    squares = lax.optimization_barrier(jnp.mean(right * right, axis=0))
    inverse = lax.rsqrt(squares - average * average + EPS)
    centred = ((right - average) * inverse * channel_gain[:, None]).astype(jnp.bfloat16)
    blocks = centred.reshape(GROUPS, BRANCH // GROUPS, TOKENS // BLOCK, BLOCK)
    lower = jnp.tril(jnp.ones((BLOCK, BLOCK), dtype=bool))
    masked = jnp.where(lower[None], spatial, jnp.zeros_like(spatial))
    token_mix = jnp.einsum('gts,gcns->gcnt', masked.astype(jnp.float32), blocks.astype(jnp.float32))
    token_mix = token_mix + spatial_bias[:, None, None, :]
    gated = (left * token_mix.reshape(BRANCH, TOKENS)).astype(jnp.bfloat16)
    total = block_sum(mixer_out, mixer_out_scale, gated)
    stream = (stream.astype(jnp.float32) + total).astype(jnp.bfloat16)
    return half_step(stream, second_gain, second_gate, second_gate_scale, second_up, second_up_scale, second_down, second_down_scale)
```

```python
import functools

import jax
import jax.numpy as jnp
from jax import lax
from jax.experimental import pallas as pl
from jax.experimental.pallas import tpu as pltpu
from jax.sharding import PartitionSpec as P

EPS = 1e-06
F32 = jnp.float32
BF16 = jnp.bfloat16
LANES = 128


def rotate(value, axis, by):
    size = lax.axis_size(axis)
    return lax.ppermute(value, axis, [(i, (i + by) % size) for i in range(size)])


def swap_cores(value):
    return lax.ppermute(value, "tp", [(i, i ^ 1) for i in range(lax.axis_size("tp"))])


def place(whole, part, at, row):
    return lax.dynamic_update_slice(whole, part[None], (at, jnp.uint32(row), jnp.uint32(0)))


def ahead(me, by, size):
    return lax.rem(me + jnp.uint32(by % size), jnp.uint32(size))


def ring(streams):
    size = lax.axis_size("fs")
    me = lax.axis_index("fs").astype(jnp.uint32)
    rows = [s.shape[0] for s in streams]
    starts = [sum(rows[:k]) for k in range(len(rows))]
    whole = jnp.zeros((size, sum(rows), LANES), BF16)
    for s, row in zip(streams, starts):
        whole = place(whole, s, me, row)
    ups, downs = list(streams), list(streams)
    for step in range(1, size // 2):
        for k, row in enumerate(starts):
            ups[k] = rotate(ups[k], "fs", 1)
            downs[k] = rotate(downs[k], "fs", -1)
            whole = place(whole, ups[k], ahead(me, -step, size), row)
            whole = place(whole, downs[k], ahead(me, step, size), row)
    far = ahead(me, size // 2, size)
    for k, row in enumerate(starts):
        half = rows[k] // 32 * 16
        whole = place(whole, rotate(ups[k][:half], "fs", 1), far, row)
        whole = place(whole, rotate(downs[k][half:], "fs", -1), far, row + half)
    return whole


def gather_tp(mine):
    back = rotate(mine, "tp", 2)
    front = rotate(mine, "tp", -2)
    far = rotate(mine, "tp", 4)
    same = jnp.stack([mine, front, far, back])
    return same, swap_cores(same)


def scatter_tp(keep, give):
    chips = keep.shape[0]
    here = lax.axis_index("tp").astype(jnp.uint32) // 2
    both = keep.astype(F32) + swap_cores(give).astype(F32)

    def block(d):
        return lax.dynamic_index_in_dim(both, ahead(here, d, chips), 0, keepdims=False).astype(BF16)

    own = lax.dynamic_index_in_dim(both, here, 0, keepdims=False)
    a = rotate(block(1), "tp", 2)
    b = rotate(block(3), "tp", -2)
    c = rotate(block(2), "tp", 4)
    return own + a.astype(F32) + b.astype(F32) + c.astype(F32)


def scale_rows(scale):
    hi = lax.reduce_precision(scale, 8, 7)
    rest = scale - hi
    mid = lax.reduce_precision(rest, 8, 7)
    rows = jnp.stack([hi, mid, rest - mid])
    return jnp.pad(rows, ((0, 13), (0, 0))).astype(BF16)


def nt(a, b):
    return lax.dot_general(a, b, (((1,), (1,)), ((), ())), preferred_element_type=F32)


def nn(a, b):
    return lax.dot_general(a, b, (((1,), (0,)), ((), ())), preferred_element_type=F32)


def chunks_of(n, step=256):
    return [(at, min(step, n - at)) for at in range(0, n, step)]


def normalise(place_ref, same_ref, other_ref, gain_ref, raw, xn):
    chips, tokens, width = same_ref.shape
    here, core = place_ref[0], place_ref[1]
    for d in range(chips):
        chip = (here + d) % chips
        raw[2 * chip + core] = same_ref[d]
        raw[2 * chip + 1 - core] = other_ref[d]
    total = jnp.zeros((tokens, 1), F32)
    for j in range(2 * chips):
        v = raw[j].astype(F32)
        total = total + jnp.sum(v * v, axis=1, keepdims=True)
    inverse = lax.rsqrt(total / (2 * chips * width) + EPS)
    for j in range(2 * chips):
        v = raw[j].astype(F32)
        xn[:, j * width : (j + 1) * width] = (v * inverse * gain_ref[:, j * width : (j + 1) * width]).astype(BF16)


def lanes(ref, row, n, first, count):
    return jnp.concatenate([ref[f, row : row + n, :] for f in range(first, first + count)], axis=1)


def emit(core, hid, w, row, hidden, scale_row, keep_ref, give_ref):
    per = keep_ref.shape[2] // LANES
    for k in range(keep_ref.shape[0]):
        pair = []
        for c in range(2):
            f = (2 * k + c) * per
            s = lanes(w, scale_row, 16, f, per).astype(F32)
            s = jnp.sum(s, axis=0, keepdims=True)
            pair.append((nn(hid, lanes(w, row, hidden, f, per)) * s).astype(BF16))
        keep_ref[k] = jnp.where(core == 0, pair[0], pair[1])
        give_ref[k] = jnp.where(core == 0, pair[1], pair[0])


def feed_body(place_ref, same_ref, other_ref, gain_ref, gs_ref, us_ref, w_hbm, keep_ref, give_ref, w, raw, xn, hid, sems, *, hidden):
    pieces = []
    for at, n in chunks_of(hidden):
        pieces += [(at, n), (hidden + at, n)]
    pieces.append((2 * hidden, w.shape[1] - 2 * hidden))
    copies = [
        pltpu.make_async_copy(w_hbm.at[:, pl.ds(at, n), :], w.at[:, pl.ds(at, n), :], sems.at[k])
        for k, (at, n) in enumerate(pieces)
    ]
    for c in copies:
        c.start()
    normalise(place_ref, same_ref, other_ref, gain_ref, raw, xn)
    x = xn[...]
    count = w.shape[0]
    for k, (at, n) in enumerate(chunks_of(hidden)):
        copies[2 * k].wait()
        copies[2 * k + 1].wait()
        g = nt(x, lanes(w, at, n, 0, count)) * gs_ref[:, at : at + n]
        u = nt(x, lanes(w, hidden + at, n, 0, count)) * us_ref[:, at : at + n]
        hid[:, at : at + n] = (g / (1.0 + jnp.exp(-g)) * u).astype(BF16)
    copies[-1].wait()
    emit(place_ref[1], hid[...], w, 2 * hidden, hidden, 3 * hidden, keep_ref, give_ref)


VMEM = pl.BlockSpec(memory_space=pltpu.VMEM)
SMEM = pl.BlockSpec(memory_space=pltpu.SMEM)
HBM = pl.BlockSpec(memory_space=pltpu.HBM)


def feed(where, same, other, gain, gate_scale, up_scale, w):
    chips, tokens, width = same.shape
    hidden = gate_scale.shape[0]
    wide = 2 * chips * width
    out = jax.ShapeDtypeStruct(same.shape, BF16)
    flops = 2 * tokens * 3 * hidden * wide
    return pl.pallas_call(
        functools.partial(feed_body, hidden=hidden),
        out_shape=(out, out),
        in_specs=[SMEM, VMEM, VMEM, VMEM, VMEM, VMEM, HBM],
        out_specs=(VMEM, VMEM),
        scratch_shapes=[
            pltpu.VMEM(w.shape, BF16),
            pltpu.VMEM((2 * chips, tokens, width), BF16),
            pltpu.VMEM((tokens, wide), BF16),
            pltpu.VMEM((tokens, hidden), BF16),
            pltpu.SemaphoreType.DMA((2 * len(chunks_of(hidden)) + 1,)),
        ],
        compiler_params=pltpu.CompilerParams(vmem_limit_bytes=56 * 1024 * 1024),
        cost_estimate=pl.CostEstimate(flops=flops, bytes_accessed=2 * w.size, transcendentals=tokens * hidden),
        name="feed",
    )(where, same, other, gain[None], gate_scale[None], up_scale[None], w)


def gelu(t):
    return 0.5 * t * (1.0 + jnp.tanh(0.7978845608028654 * (t + 0.044715 * t * t * t)))


def branch_body(place_ref, same_ref, other_ref, gain_ref, ls_ref, rs_ref, w_ref, left_ref, right_ref, stat_ref, raw, xn):
    normalise(place_ref, same_ref, other_ref, gain_ref, raw, xn)
    n = left_ref.shape[1]
    both = nt(xn[...], lanes(w_ref, 0, 2 * n, 0, w_ref.shape[0]))
    left_ref[...] = gelu(both[:, :n] * ls_ref[...])
    right = gelu(both[:, n:] * rs_ref[...])
    right_ref[...] = right
    sums = jnp.sum(right, axis=1, keepdims=True)
    squares = jnp.sum(right * right, axis=1, keepdims=True)
    column = lax.broadcasted_iota(jnp.int32, stat_ref.shape, 1)
    stat_ref[...] = jnp.where(column == 0, sums, squares)


def branch(where, same, other, gain, left_scale, right_scale, w):
    chips, tokens, width = same.shape
    n = left_scale.shape[0]
    part = jax.ShapeDtypeStruct((tokens, n), F32)
    return pl.pallas_call(
        branch_body,
        out_shape=(part, part, jax.ShapeDtypeStruct((tokens, LANES), F32)),
        in_specs=[SMEM] + [VMEM] * 6,
        out_specs=(VMEM, VMEM, VMEM),
        scratch_shapes=[
            pltpu.VMEM((2 * chips, tokens, width), BF16),
            pltpu.VMEM((tokens, 2 * chips * width), BF16),
        ],
        compiler_params=pltpu.CompilerParams(vmem_limit_bytes=40 * 1024 * 1024),
        cost_estimate=pl.CostEstimate(flops=2 * tokens * 2 * n * 2 * chips * width, bytes_accessed=2 * w.size, transcendentals=2 * tokens * n),
        name="branch",
    )(where, same, other, gain[None], left_scale[None], right_scale[None], w)


def mix_body(place_ref, left_ref, right_ref, stat_ref, gain_ref, spatial_ref, bias_ref, w_ref, keep_ref, give_ref, gated, *, channels):
    tokens, n = left_ref.shape
    groups, span, _ = spatial_ref.shape
    each = n // groups
    mean = stat_ref[:, 0:1] / channels
    inverse = lax.rsqrt(stat_ref[:, 1:2] / channels - mean * mean + EPS)
    centred = ((right_ref[...] - mean) * inverse * gain_ref[...]).astype(BF16)
    target = lax.broadcasted_iota(jnp.int32, (span, span), 0)
    source = lax.broadcasted_iota(jnp.int32, (span, span), 1)
    for g in range(groups):
        causal = jnp.where(source <= target, spatial_ref[g].astype(F32), 0.0).astype(BF16)
        for b in range(tokens // span):
            at, to = b * span, g * each
            mixed = nn(causal, centred[at : at + span, to : to + each]) + bias_ref[:, g : g + 1]
            gated[at : at + span, to : to + each] = (left_ref[at : at + span, to : to + each] * mixed).astype(BF16)
    emit(place_ref[1], gated[...], w_ref, 2 * n, n, 3 * n, keep_ref, give_ref)


def mix(where, left, right, stat, gain, spatial, bias, w, shape):
    tokens, n = left.shape
    out = jax.ShapeDtypeStruct(shape, BF16)
    return pl.pallas_call(
        functools.partial(mix_body, channels=n * 2 * shape[0]),
        out_shape=(out, out),
        in_specs=[SMEM] + [VMEM] * 7,
        out_specs=(VMEM, VMEM),
        scratch_shapes=[pltpu.VMEM((tokens, n), BF16)],
        compiler_params=pltpu.CompilerParams(vmem_limit_bytes=40 * 1024 * 1024),
        cost_estimate=pl.CostEstimate(flops=2 * tokens * n * 2 * shape[0] * shape[2], bytes_accessed=2 * w.size, transcendentals=0),
        name="mix",
    )(where, left, right, stat, gain[None], spatial, bias.T, w)


def sum_tp(stat):
    flat = stat.T
    flat = flat + swap_cores(flat)
    flat = flat + rotate(flat, "tp", 4)
    flat = flat + rotate(flat, "tp", 2)
    return flat.T


def local(
    stream,
    first_gain,
    first_gate,
    first_gate_scale,
    first_up,
    first_up_scale,
    first_down,
    first_down_scale,
    mixer_gain,
    mixer_left,
    mixer_left_scale,
    mixer_right,
    mixer_right_scale,
    channel_gain,
    spatial,
    spatial_bias,
    mixer_out,
    mixer_out_scale,
    second_gain,
    second_gate,
    second_gate_scale,
    second_up,
    second_up_scale,
    second_down,
    second_down_scale,
):
    tp = lax.axis_index("tp").astype(jnp.uint32)
    where = jnp.stack([tp // 2, tp % 2]).astype(jnp.int32)
    hidden = first_gate.shape[1]

    def packed(gate, up, down, scale):
        return [gate.T.astype(BF16), up.T.astype(BF16), down.astype(BF16), scale_rows(scale)]

    g1, u1, d1, s1 = packed(first_gate, first_up, first_down, first_down_scale)
    cut = 256
    one = ring([jnp.concatenate([g1, u1[:cut]]), jnp.concatenate([u1[cut:], d1, s1])])
    two = lax.all_gather(jnp.concatenate(packed(mixer_left, mixer_right, mixer_out, mixer_out_scale)), "fs")
    three = lax.all_gather(jnp.concatenate(packed(second_gate, second_up, second_down, second_down_scale)), "fs")

    rest = stream.T
    same, other = gather_tp(rest)
    keep, give = feed(where, same, other, first_gain, first_gate_scale, first_up_scale, one)
    rest = (rest.astype(F32) + 0.5 * scatter_tp(keep, give)).astype(BF16)

    same, other = gather_tp(rest)
    left, right, stat = branch(where, same, other, mixer_gain, mixer_left_scale, mixer_right_scale, two)
    stat = sum_tp(stat[:, :2])
    keep, give = mix(where, left, right, stat, channel_gain, spatial, spatial_bias, two, same.shape)
    rest = (rest.astype(F32) + scatter_tp(keep, give)).astype(BF16)

    same, other = gather_tp(rest)
    keep, give = feed(where, same, other, second_gain, second_gate_scale, second_up_scale, three)
    return (rest.astype(F32) + 0.5 * scatter_tp(keep, give)).astype(BF16).T


def solution(mesh):
    return jax.shard_map(
        local,
        mesh=mesh,
        in_specs=(
            P("tp", ("grp", "fs")),
            P(),
            P("fs", "tp"),
            P("tp"),
            P("fs", "tp"),
            P("tp"),
            P("tp", "fs"),
            P("fs"),
            P(),
            P("fs", "tp"),
            P("tp"),
            P("fs", "tp"),
            P("tp"),
            P("tp"),
            P("tp", None, None),
            P("tp", None),
            P("tp", "fs"),
            P("fs"),
            P(),
            P("fs", "tp"),
            P("tp"),
            P("fs", "tp"),
            P("tp"),
            P("tp", "fs"),
            P("fs"),
        ),
        out_specs=P("tp", ("grp", "fs")),
        check_vma=False,
    )
```

```python
import functools

import jax
import jax.numpy as jnp
from jax import lax
from jax.experimental import pallas as pl
from jax.experimental.pallas import tpu as pltpu
from jax.sharding import PartitionSpec as P

EPS = 1e-06
F32 = jnp.float32
BF16 = jnp.bfloat16
LANES = 128


def rotate(value, axis, by):
    size = lax.axis_size(axis)
    return lax.ppermute(value, axis, [(i, (i + by) % size) for i in range(size)])


def swap_cores(value):
    return lax.ppermute(value, "tp", [(i, i ^ 1) for i in range(lax.axis_size("tp"))])


def ahead(me, by, size):
    return lax.rem(me + jnp.uint32(by % size), jnp.uint32(size))


def swap_groups(value):
    return lax.ppermute(value, "grp", [(i, i ^ 1) for i in range(lax.axis_size("grp"))])


def ring(shard):
    size = lax.axis_size("fs")
    odd = lax.axis_index("grp").astype(jnp.uint32) % 2
    halves = shard.reshape(2, shard.shape[0] // 2, LANES)
    mine = lax.dynamic_index_in_dim(halves, odd, 0, keepdims=False)
    pieces = []
    up = down = mine
    for _ in range(1, size // 2):
        up = rotate(up, "fs", 1)
        down = rotate(down, "fs", -1)
        both = jnp.stack([up, down])
        pieces += [both, swap_groups(both)]
    half = mine.shape[0] // 32 * 16
    far = jnp.concatenate([rotate(up[:half], "fs", 1), rotate(down[half:], "fs", -1)])[None]
    return [shard[None], *pieces, far, swap_groups(far)]


def gather_tp(mine):
    back = rotate(mine, "tp", 2)
    front = rotate(mine, "tp", -2)
    far = rotate(mine, "tp", 4)
    same = jnp.stack([mine, front, far, back])
    return same, swap_cores(same)


def scatter_tp(keep, give):
    chips = keep.shape[0]
    here = lax.axis_index("tp").astype(jnp.uint32) // 2
    both = keep.astype(F32) + swap_cores(give).astype(F32)

    def block(d):
        return lax.dynamic_index_in_dim(both, ahead(here, d, chips), 0, keepdims=False).astype(BF16)

    own = lax.dynamic_index_in_dim(both, here, 0, keepdims=False)
    a = rotate(block(1), "tp", 2)
    b = rotate(block(3), "tp", -2)
    c = rotate(block(2), "tp", 4)
    return own + a.astype(F32) + b.astype(F32) + c.astype(F32)


def scale_rows(scale, rows):
    hi = lax.reduce_precision(scale, 8, 7)
    rest = scale - hi
    mid = lax.reduce_precision(rest, 8, 7)
    parts = jnp.stack([hi, mid, rest - mid])
    return jnp.pad(parts, ((0, rows - 3), (0, 0))).astype(BF16)


def nt(a, b):
    return lax.dot_general(a, b, (((1,), (1,)), ((), ())), preferred_element_type=F32)


def nn(a, b):
    return lax.dot_general(a, b, (((1,), (0,)), ((), ())), preferred_element_type=F32)


def chunks_of(n, step=256):
    return [(at, min(step, n - at)) for at in range(0, n, step)]


def normalise(place_ref, same_ref, other_ref, vec_ref, at, raw, xn):
    chips, tokens, width = same_ref.shape
    here, core = place_ref[0], place_ref[1]
    for d in range(chips):
        chip = (here + d) % chips
        raw[2 * chip + core] = same_ref[d]
        raw[2 * chip + 1 - core] = other_ref[d]
    total = jnp.zeros((tokens, 1), F32)
    for j in range(2 * chips):
        v = raw[j].astype(F32)
        total = total + jnp.sum(v * v, axis=1, keepdims=True)
    inverse = lax.rsqrt(total / (2 * chips * width) + EPS)
    for j in range(2 * chips):
        v = raw[j].astype(F32)
        xn[:, j * width : (j + 1) * width] = (v * inverse * vec_ref[:, at + j * width : at + (j + 1) * width]).astype(BF16)


def lanes(ref, row, n, first, count):
    return jnp.concatenate([ref[f, row : row + n, :] for f in range(first, first + count)], axis=1)


def emit(core, hid, w, row, hidden, scale_row, keep_ref, give_ref):
    per = keep_ref.shape[2] // LANES
    for k in range(keep_ref.shape[0]):
        pair = []
        for c in range(2):
            f = (2 * k + c) * per
            s = lanes(w, scale_row, 16, f, per).astype(F32)
            s = jnp.sum(s, axis=0, keepdims=True)
            pair.append((nn(hid, lanes(w, row, hidden, f, per)) * s).astype(BF16))
        keep_ref[k] = jnp.where(core == 0, pair[0], pair[1])
        give_ref[k] = jnp.where(core == 0, pair[1], pair[0])


def assemble(place_ref, pieces, w, row):
    count = w.shape[0]
    me, odd = place_ref[2], place_ref[3]
    half = pieces[1].shape[1]
    w[me, row:, :] = pieces[0][0]
    for step in range(1, len(pieces) // 2 + 1):
        ours, theirs = pieces[2 * step - 1], pieces[2 * step]
        for k in range(ours.shape[0]):
            f = (me + (count - step if k == 0 else step)) % count
            a, b = ours[k], theirs[k]
            w[f, row : row + half, :] = jnp.where(odd == 0, a, b)
            w[f, row + half :, :] = jnp.where(odd == 0, b, a)


def feed_body(*refs, hidden, offsets, gate_row, ring_pieces):
    place_ref, same_ref, other_ref, vec_ref, w_hbm = refs[:5]
    pieces = refs[5 : 5 + ring_pieces]
    keep_ref, give_ref, w, raw, xn, hid, sems = refs[5 + ring_pieces :]
    gain_at, gate_at, up_at = offsets
    count, rows, _ = w.shape
    parts = []
    for at, n in chunks_of(hidden):
        parts.append([at] if ring_pieces else [at, hidden + at])
    moves = [(at, n) for (at, n), ats in zip(chunks_of(hidden), parts) for at in ats]
    if not ring_pieces:
        moves.append((2 * hidden, rows - 2 * hidden))
    copies = [
        pltpu.make_async_copy(w_hbm.at[:, pl.ds(gate_row + at, n), :], w.at[:, pl.ds(at, n), :], sems.at[k])
        for k, (at, n) in enumerate(
            (at, n)
            for j, (_, size) in enumerate(chunks_of(hidden))
            for at, n in [(a, size) for a in parts[j]]
        )
    ]
    if not ring_pieces:
        at, n = moves[-1]
        copies.append(
            pltpu.make_async_copy(w_hbm.at[:, pl.ds(gate_row + at, n), :], w.at[:, pl.ds(at, n), :], sems.at[len(copies)])
        )
    for c in copies:
        c.start()
    if ring_pieces:
        assemble(place_ref, pieces, w, hidden)
    normalise(place_ref, same_ref, other_ref, vec_ref, gain_at, raw, xn)
    x = xn[...]
    done = 0
    for j, (at, n) in enumerate(chunks_of(hidden)):
        for _ in parts[j]:
            copies[done].wait()
            done += 1
        g = nt(x, lanes(w, at, n, 0, count)) * vec_ref[:, gate_at + at : gate_at + at + n]
        u = nt(x, lanes(w, hidden + at, n, 0, count)) * vec_ref[:, up_at + at : up_at + at + n]
        hid[:, at : at + n] = (g / (1.0 + jnp.exp(-g)) * u).astype(BF16)
    for c in copies[done:]:
        c.wait()
    emit(place_ref[1], hid[...], w, 2 * hidden, hidden, 3 * hidden, keep_ref, give_ref)


VMEM = pl.BlockSpec(memory_space=pltpu.VMEM)
SMEM = pl.BlockSpec(memory_space=pltpu.SMEM)
HBM = pl.BlockSpec(memory_space=pltpu.HBM)


def feed(where, same, other, vec, offsets, hidden, w, gate_row, pieces=()):
    chips, tokens, width = same.shape
    wide = 2 * chips * width
    rows = hidden + pieces[0].shape[1] if pieces else w.shape[1]
    out = jax.ShapeDtypeStruct(same.shape, BF16)
    return pl.pallas_call(
        functools.partial(feed_body, hidden=hidden, offsets=offsets, gate_row=gate_row, ring_pieces=len(pieces)),
        out_shape=(out, out),
        in_specs=[SMEM, VMEM, VMEM, VMEM, HBM] + [VMEM] * len(pieces),
        out_specs=(VMEM, VMEM),
        scratch_shapes=[
            pltpu.VMEM((w.shape[0], rows, LANES), BF16),
            pltpu.VMEM((2 * chips, tokens, width), BF16),
            pltpu.VMEM((tokens, wide), BF16),
            pltpu.VMEM((tokens, hidden), BF16),
            pltpu.SemaphoreType.DMA((2 * len(chunks_of(hidden)) + 1,)),
        ],
        compiler_params=pltpu.CompilerParams(vmem_limit_bytes=36 * 1024 * 1024),
        cost_estimate=pl.CostEstimate(
            flops=6 * tokens * hidden * wide, bytes_accessed=2 * w.shape[0] * rows * LANES, transcendentals=tokens * hidden
        ),
        name="feed",
    )(where, same, other, vec, w, *pieces)


def gelu(t):
    return 0.5 * t * (1.0 + jnp.tanh(0.7978845608028654 * (t + 0.044715 * t * t * t)))


def branch_body(place_ref, same_ref, other_ref, vec_ref, w_hbm, left_ref, right_ref, stat_ref, raw, xn, w, sem, *, offsets):
    gain_at, left_at, right_at = offsets
    n = left_ref.shape[1]
    copy = pltpu.make_async_copy(w_hbm.at[:, pl.ds(0, 2 * n), :], w, sem)
    copy.start()
    normalise(place_ref, same_ref, other_ref, vec_ref, gain_at, raw, xn)
    copy.wait()
    both = nt(xn[...], lanes(w, 0, 2 * n, 0, w.shape[0]))
    left_ref[...] = gelu(both[:, :n] * vec_ref[:, left_at : left_at + n])
    right = gelu(both[:, n:] * vec_ref[:, right_at : right_at + n])
    right_ref[...] = right
    sums = jnp.sum(right, axis=1, keepdims=True)
    squares = jnp.sum(right * right, axis=1, keepdims=True)
    column = lax.broadcasted_iota(jnp.int32, right.shape, 1)
    stat_ref[...] = jnp.where(column == 0, sums, squares).T[: stat_ref.shape[0]]


def branch(where, same, other, vec, offsets, n, w):
    chips, tokens, width = same.shape
    part = jax.ShapeDtypeStruct((tokens, n), F32)
    return pl.pallas_call(
        functools.partial(branch_body, offsets=offsets),
        out_shape=(part, part, jax.ShapeDtypeStruct((8, tokens), F32)),
        in_specs=[SMEM, VMEM, VMEM, VMEM, HBM],
        out_specs=(VMEM, VMEM, VMEM),
        scratch_shapes=[
            pltpu.VMEM((2 * chips, tokens, width), BF16),
            pltpu.VMEM((tokens, 2 * chips * width), BF16),
            pltpu.VMEM((w.shape[0], 2 * n, LANES), BF16),
            pltpu.SemaphoreType.DMA,
        ],
        compiler_params=pltpu.CompilerParams(vmem_limit_bytes=16 * 1024 * 1024),
        cost_estimate=pl.CostEstimate(
            flops=4 * tokens * n * 2 * chips * width, bytes_accessed=8 * n * chips * width, transcendentals=2 * tokens * n
        ),
        name="branch",
    )(where, same, other, vec, w)


def mix_body(place_ref, left_ref, right_ref, stat_ref, vec_ref, spatial_ref, w_hbm, keep_ref, give_ref, gated, w, sem, *, offsets, channels):
    gain_at, bias_at = offsets
    tokens, n = left_ref.shape
    groups, span, _ = spatial_ref.shape
    each = n // groups
    copy = pltpu.make_async_copy(w_hbm.at[:, pl.ds(2 * n, w.shape[1]), :], w, sem)
    copy.start()
    lines = jnp.concatenate([stat_ref[...], jnp.zeros((LANES - stat_ref.shape[0], tokens), F32)]).T
    mean = lines[:, 0:1] / channels
    inverse = lax.rsqrt(lines[:, 1:2] / channels - mean * mean + EPS)
    centred = ((right_ref[...] - mean) * inverse * vec_ref[:, gain_at : gain_at + n]).astype(BF16)
    target = lax.broadcasted_iota(jnp.int32, (span, span), 0)
    source = lax.broadcasted_iota(jnp.int32, (span, span), 1)
    for g in range(groups):
        causal = jnp.where(source <= target, spatial_ref[g].astype(F32), 0.0).astype(BF16)
        bias = jnp.broadcast_to(vec_ref[:, bias_at + g * span : bias_at + (g + 1) * span], (LANES, span)).T[:, 0:1]
        for b in range(tokens // span):
            at, to = b * span, g * each
            mixed = nn(causal, centred[at : at + span, to : to + each]) + bias
            gated[at : at + span, to : to + each] = (left_ref[at : at + span, to : to + each] * mixed).astype(BF16)
    copy.wait()
    emit(place_ref[1], gated[...], w, 0, n, n, keep_ref, give_ref)


def mix(where, left, right, stat, vec, offsets, spatial, w, rows, shape):
    tokens, n = left.shape
    out = jax.ShapeDtypeStruct(shape, BF16)
    return pl.pallas_call(
        functools.partial(mix_body, offsets=offsets, channels=n * 2 * shape[0]),
        out_shape=(out, out),
        in_specs=[SMEM] + [VMEM] * 5 + [HBM],
        out_specs=(VMEM, VMEM),
        scratch_shapes=[
            pltpu.VMEM((tokens, n), BF16),
            pltpu.VMEM((w.shape[0], rows - 2 * n, LANES), BF16),
            pltpu.SemaphoreType.DMA,
        ],
        compiler_params=pltpu.CompilerParams(vmem_limit_bytes=16 * 1024 * 1024),
        cost_estimate=pl.CostEstimate(
            flops=4 * tokens * n * shape[0] * shape[2], bytes_accessed=4 * n * shape[0] * shape[2], transcendentals=0
        ),
        name="mix",
    )(where, left, right, stat, vec, spatial, w)


def sum_tp(stat):
    stat = stat + swap_cores(stat)
    stat = stat + rotate(stat, "tp", 4)
    return stat + rotate(stat, "tp", 2)


def in_a_row(vectors):
    padded = [jnp.pad(v, (0, -v.shape[0] % LANES)) for v in vectors]
    starts = [sum(p.shape[0] for p in padded[:k]) for k in range(len(padded))]
    return jnp.concatenate(padded)[None], starts


def local(
    stream,
    first_gain,
    first_gate,
    first_gate_scale,
    first_up,
    first_up_scale,
    first_down,
    first_down_scale,
    mixer_gain,
    mixer_left,
    mixer_left_scale,
    mixer_right,
    mixer_right_scale,
    channel_gain,
    spatial,
    spatial_bias,
    mixer_out,
    mixer_out_scale,
    second_gain,
    second_gate,
    second_gate_scale,
    second_up,
    second_up_scale,
    second_down,
    second_down_scale,
):
    tp = lax.axis_index("tp").astype(jnp.uint32)
    spots = [tp // 2, tp % 2, lax.axis_index("fs"), lax.axis_index("grp").astype(jnp.uint32) % 2]
    where = jnp.stack([i.astype(jnp.int32) for i in spots])
    hidden = first_gate.shape[1]
    n = mixer_left.shape[1]
    gates = [
        mixer_left.T.astype(BF16),
        mixer_right.T.astype(BF16),
        mixer_out.astype(BF16),
        scale_rows(mixer_out_scale, 16),
        first_gate.T.astype(BF16),
    ]
    branch_rows = 3 * n + 16
    one = ring(jnp.concatenate([first_up.T.astype(BF16), first_down.astype(BF16), scale_rows(first_down_scale, 32)]))
    two = lax.all_gather(jnp.concatenate(gates), "fs")
    second = [
        second_gate.T.astype(BF16),
        second_up.T.astype(BF16),
        second_down.astype(BF16),
        scale_rows(second_down_scale, 16),
    ]
    three = lax.all_gather(jnp.concatenate(second), "fs")
    vec, at = in_a_row(
        [
            first_gain,
            first_gate_scale,
            first_up_scale,
            mixer_gain,
            mixer_left_scale,
            mixer_right_scale,
            channel_gain,
            spatial_bias.reshape(-1),
            second_gain,
            second_gate_scale,
            second_up_scale,
        ]
    )

    rest = stream.T
    same, other = gather_tp(rest)
    keep, give = feed(where, same, other, vec, at[0:3], hidden, two, branch_rows, one)
    rest = (rest.astype(F32) + 0.5 * scatter_tp(keep, give)).astype(BF16)

    same, other = gather_tp(rest)
    left, right, stat = branch(where, same, other, vec, at[3:6], n, two)
    keep, give = mix(where, left, right, sum_tp(stat), vec, at[6:8], spatial, two, branch_rows, same.shape)
    rest = (rest.astype(F32) + scatter_tp(keep, give)).astype(BF16)

    same, other = gather_tp(rest)
    keep, give = feed(where, same, other, vec, at[8:11], hidden, three, 0)
    return (rest.astype(F32) + 0.5 * scatter_tp(keep, give)).astype(BF16).T


def solution(mesh):
    return jax.shard_map(
        local,
        mesh=mesh,
        in_specs=(
            P("tp", ("grp", "fs")),
            P(),
            P("fs", "tp"),
            P("tp"),
            P("fs", "tp"),
            P("tp"),
            P("tp", "fs"),
            P("fs"),
            P(),
            P("fs", "tp"),
            P("tp"),
            P("fs", "tp"),
            P("tp"),
            P("tp"),
            P("tp", None, None),
            P("tp", None),
            P("tp", "fs"),
            P("fs"),
            P(),
            P("fs", "tp"),
            P("tp"),
            P("fs", "tp"),
            P("tp"),
            P("tp", "fs"),
            P("fs"),
        ),
        out_specs=P("tp", ("grp", "fs")),
        check_vma=False,
    )
```

```python
import functools

import jax
import jax.numpy as jnp
from jax import lax
from jax.experimental import pallas as pl
from jax.experimental.pallas import tpu as pltpu
from jax.sharding import PartitionSpec as P

EPS = 1e-06
F32 = jnp.float32
BF16 = jnp.bfloat16
LANES = 128
VMEM = pl.BlockSpec(memory_space=pltpu.VMEM)
SMEM = pl.BlockSpec(memory_space=pltpu.SMEM)
HBM = pl.BlockSpec(memory_space=pltpu.HBM)


def rotate(value, axis, by):
    size = lax.axis_size(axis)
    return lax.ppermute(value, axis, [(i, (i + by) % size) for i in range(size)])


def swap_cores(value):
    return lax.ppermute(value, "tp", [(i, i ^ 1) for i in range(lax.axis_size("tp"))])


def ahead(me, by, size):
    return lax.rem(me + jnp.uint32(by % size), jnp.uint32(size))


def swap_groups(value):
    return lax.ppermute(value, "grp", [(i, i ^ 1) for i in range(lax.axis_size("grp"))])


def ring(shard, stream, half):
    size = lax.axis_size("fs")
    pieces = [shard]
    up = down = stream
    for _ in range(1, size // 2):
        up = rotate(up, "fs", 1)
        down = rotate(down, "fs", -1)
        pieces += [up, down, swap_groups(jnp.stack([up[:half], down[:half]]))]
    cut = stream.shape[0] // 32 * 16
    far = jnp.concatenate([rotate(up[:cut], "fs", 1), rotate(down[cut:], "fs", -1)])
    return [*pieces, far, swap_groups(far[None, :half])]


def gather_tp(mine):
    back = rotate(mine, "tp", 2)
    front = rotate(mine, "tp", -2)
    far = rotate(mine, "tp", 4)
    same = jnp.stack([mine, front, far, back])
    return same, swap_cores(same)


def scatter_tp(keep, give):
    chips = keep.shape[0]
    here = lax.axis_index("tp").astype(jnp.uint32) // 2
    both = keep.astype(F32) + swap_cores(give).astype(F32)

    def block(d):
        return lax.dynamic_index_in_dim(both, ahead(here, d, chips), 0, keepdims=False).astype(BF16)

    own = lax.dynamic_index_in_dim(both, here, 0, keepdims=False)
    a = rotate(block(1), "tp", 2)
    b = rotate(block(3), "tp", -2)
    c = rotate(block(2), "tp", 4)
    return own + a.astype(F32) + b.astype(F32) + c.astype(F32)


def put(ref, row, parts):
    for part, rows in parts:
        v = part[...]
        if v.shape[0] == 1:
            hi = v.astype(BF16)
            mid = (v - hi.astype(F32)).astype(BF16)
            low = (v - hi.astype(F32) - mid.astype(F32)).astype(BF16)
            line = lax.broadcasted_iota(jnp.int32, (rows, LANES), 0)
            hi, mid, low = (jnp.broadcast_to(t.astype(F32), (rows, LANES)) for t in (hi, mid, low))
            v = jnp.where(line == 0, hi, jnp.where(line == 1, mid, jnp.where(line == 2, low, 0.0)))
        ref[row : row + rows, :] = v.astype(BF16)
        row += rows


def pack_first_body(place_ref, left, right, out, out_scale, gate, up, down, down_scale, shard_ref, stream_ref, two_ref, *, half):
    put(two_ref, 0, [(left, LANES), (right, LANES), (out, out.shape[0]), (out_scale, 16), (gate, gate.shape[0])])
    put(shard_ref, 0, [(up, up.shape[0]), (down, down.shape[0]), (down_scale, 32)])
    odd = place_ref[3]
    stream_ref[:half] = jnp.where(odd == 0, shard_ref[:half], shard_ref[half : 2 * half])
    stream_ref[half:] = shard_ref[2 * half :]


def pack_first(where, left, right, out, out_scale, gate, up, down, down_scale):
    rows = up.shape[0] + down.shape[0] + 32
    half = rows // 48 * 16
    two_rows = 2 * LANES + out.shape[0] + 16 + gate.shape[0]
    shapes = [jax.ShapeDtypeStruct((n, LANES), BF16) for n in (rows, rows - half, two_rows)]
    packed = pl.pallas_call(
        functools.partial(pack_first_body, half=half),
        out_shape=shapes,
        in_specs=[SMEM] + [VMEM] * 8,
        out_specs=[VMEM] * 3,
        compiler_params=pltpu.CompilerParams(vmem_limit_bytes=8 * 1024 * 1024),
        name="pack_first",
    )(where, left, right, out, out_scale[None], gate, up, down, down_scale[None])
    return (*packed, half)


def pack_second_body(gate, up, down, down_scale, three_ref):
    put(three_ref, 0, [(gate, gate.shape[0]), (up, up.shape[0]), (down, down.shape[0]), (down_scale, 16)])


def pack_second(gate, up, down, down_scale):
    rows = gate.shape[0] + up.shape[0] + down.shape[0] + 16
    return pl.pallas_call(
        pack_second_body,
        out_shape=jax.ShapeDtypeStruct((rows, LANES), BF16),
        in_specs=[VMEM] * 4,
        out_specs=VMEM,
        compiler_params=pltpu.CompilerParams(vmem_limit_bytes=8 * 1024 * 1024),
        name="pack_second",
    )(gate, up, down, down_scale[None])


def nt(a, b):
    return lax.dot_general(a, b, (((1,), (1,)), ((), ())), preferred_element_type=F32)


def nn(a, b):
    return lax.dot_general(a, b, (((1,), (0,)), ((), ())), preferred_element_type=F32)


def chunks_of(n, step=256):
    return [(at, min(step, n - at)) for at in range(0, n, step)]


def normalise(place_ref, same_ref, other_ref, vec_ref, at, raw, xn):
    chips, tokens, width = same_ref.shape
    here, core = place_ref[0], place_ref[1]
    for d in range(chips):
        chip = (here + d) % chips
        raw[2 * chip + core] = same_ref[d]
        raw[2 * chip + 1 - core] = other_ref[d]
    total = jnp.zeros((tokens, 1), F32)
    for j in range(2 * chips):
        v = raw[j].astype(F32)
        total = total + jnp.sum(v * v, axis=1, keepdims=True)
    inverse = lax.rsqrt(total / (2 * chips * width) + EPS)
    for j in range(2 * chips):
        v = raw[j].astype(F32)
        xn[:, j * width : (j + 1) * width] = (v * inverse * vec_ref[:, at + j * width : at + (j + 1) * width]).astype(BF16)


def lanes(ref, row, n, first, count):
    return jnp.concatenate([ref[f, row : row + n, :] for f in range(first, first + count)], axis=1)


def emit(core, hid, w, row, hidden, scale_row, keep_ref, give_ref):
    per = keep_ref.shape[2] // LANES
    for k in range(keep_ref.shape[0]):
        pair = []
        for c in range(2):
            f = (2 * k + c) * per
            s = lanes(w, scale_row, 16, f, per).astype(F32)
            s = jnp.sum(s, axis=0, keepdims=True)
            pair.append((nn(hid, lanes(w, row, hidden, f, per)) * s).astype(BF16))
        keep_ref[k] = jnp.where(core == 0, pair[0], pair[1])
        give_ref[k] = jnp.where(core == 0, pair[1], pair[0])


def assemble(place_ref, pieces, w, row):
    count = w.shape[0]
    me, odd = place_ref[2], place_ref[3]
    half = pieces[3].shape[1]
    w[me, row:, :] = pieces[0][...]
    for step in range(1, count // 2 + 1):
        here = pieces[3 * step - 2 : 3 * step + 1]
        for k, ours in enumerate(here[:-1]):
            f = (me + (count - step if k == 0 else step)) % count
            a, b = ours[:half], here[-1][k]
            w[f, row : row + half, :] = jnp.where(odd == 0, a, b)
            w[f, row + half : row + 2 * half, :] = jnp.where(odd == 0, b, a)
            w[f, row + 2 * half :, :] = ours[half:]


def feed_body(*refs, hidden, offsets, gate_row, ring_pieces):
    place_ref, same_ref, other_ref, vec_ref, w_hbm = refs[:5]
    pieces = refs[5 : 5 + ring_pieces]
    keep_ref, give_ref, w, raw, xn, hid, sems = refs[5 + ring_pieces :]
    gain_at, gate_at, up_at = offsets
    count, rows, _ = w.shape
    parts = []
    for at, n in chunks_of(hidden):
        parts.append([at] if ring_pieces else [at, hidden + at])
    moves = [(at, n) for (at, n), ats in zip(chunks_of(hidden), parts) for at in ats]
    if not ring_pieces:
        moves.append((2 * hidden, rows - 2 * hidden))
    copies = [
        pltpu.make_async_copy(w_hbm.at[:, pl.ds(gate_row + at, n), :], w.at[:, pl.ds(at, n), :], sems.at[k])
        for k, (at, n) in enumerate(
            (at, n)
            for j, (_, size) in enumerate(chunks_of(hidden))
            for at, n in [(a, size) for a in parts[j]]
        )
    ]
    if not ring_pieces:
        at, n = moves[-1]
        copies.append(
            pltpu.make_async_copy(w_hbm.at[:, pl.ds(gate_row + at, n), :], w.at[:, pl.ds(at, n), :], sems.at[len(copies)])
        )
    for c in copies:
        c.start()
    if ring_pieces:
        assemble(place_ref, pieces, w, hidden)
    normalise(place_ref, same_ref, other_ref, vec_ref, gain_at, raw, xn)
    x = xn[...]
    done = 0
    for j, (at, n) in enumerate(chunks_of(hidden)):
        for _ in parts[j]:
            copies[done].wait()
            done += 1
        g = nt(x, lanes(w, at, n, 0, count)) * vec_ref[:, gate_at + at : gate_at + at + n]
        u = nt(x, lanes(w, hidden + at, n, 0, count)) * vec_ref[:, up_at + at : up_at + at + n]
        hid[:, at : at + n] = (g / (1.0 + jnp.exp(-g)) * u).astype(BF16)
    for c in copies[done:]:
        c.wait()
    emit(place_ref[1], hid[...], w, 2 * hidden, hidden, 3 * hidden, keep_ref, give_ref)


def feed(where, same, other, vec, offsets, hidden, w, gate_row, pieces=()):
    chips, tokens, width = same.shape
    wide = 2 * chips * width
    rows = hidden + pieces[0].shape[0] if pieces else w.shape[1]
    out = jax.ShapeDtypeStruct(same.shape, BF16)
    return pl.pallas_call(
        functools.partial(feed_body, hidden=hidden, offsets=offsets, gate_row=gate_row, ring_pieces=len(pieces)),
        out_shape=(out, out),
        in_specs=[SMEM, VMEM, VMEM, VMEM, HBM] + [VMEM] * len(pieces),
        out_specs=(VMEM, VMEM),
        scratch_shapes=[
            pltpu.VMEM((w.shape[0], rows, LANES), BF16),
            pltpu.VMEM((2 * chips, tokens, width), BF16),
            pltpu.VMEM((tokens, wide), BF16),
            pltpu.VMEM((tokens, hidden), BF16),
            pltpu.SemaphoreType.DMA((2 * len(chunks_of(hidden)) + 1,)),
        ],
        compiler_params=pltpu.CompilerParams(vmem_limit_bytes=20 * 1024 * 1024),
        cost_estimate=pl.CostEstimate(
            flops=6 * tokens * hidden * wide, bytes_accessed=2 * w.shape[0] * rows * LANES, transcendentals=tokens * hidden
        ),
        name="feed",
    )(where, same, other, vec, pltpu.with_memory_space_constraint(w, pltpu.HBM), *pieces)


def gelu(t):
    return 0.5 * t * (1.0 + jnp.tanh(0.7978845608028654 * (t + 0.044715 * t * t * t)))


def branch_body(place_ref, same_ref, other_ref, vec_ref, w_hbm, left_ref, right_ref, stat_ref, raw, xn, w, sem, *, offsets):
    gain_at, left_at, right_at = offsets
    n = left_ref.shape[1]
    copy = pltpu.make_async_copy(w_hbm.at[:, pl.ds(0, 2 * LANES), :], w, sem)
    copy.start()
    normalise(place_ref, same_ref, other_ref, vec_ref, gain_at, raw, xn)
    copy.wait()
    wide = w.shape[0] * LANES
    sides = [w[:, at : at + LANES, :].reshape(wide, n) for at in (0, LANES)]
    both = nn(xn[...], jnp.concatenate(sides, axis=1))
    left_ref[...] = gelu(both[:, :n] * vec_ref[:, left_at : left_at + n])
    right = gelu(both[:, n:] * vec_ref[:, right_at : right_at + n])
    right_ref[...] = right
    sums = jnp.sum(right, axis=1, keepdims=True)
    squares = jnp.sum(right * right, axis=1, keepdims=True)
    column = lax.broadcasted_iota(jnp.int32, right.shape, 1)
    stat_ref[...] = jnp.where(column == 0, sums, squares).T[: stat_ref.shape[0]]


def branch(where, same, other, vec, offsets, n, w):
    chips, tokens, width = same.shape
    part = jax.ShapeDtypeStruct((tokens, n), F32)
    return pl.pallas_call(
        functools.partial(branch_body, offsets=offsets),
        out_shape=(part, part, jax.ShapeDtypeStruct((8, tokens), F32)),
        in_specs=[SMEM, VMEM, VMEM, VMEM, HBM],
        out_specs=(VMEM, VMEM, VMEM),
        scratch_shapes=[
            pltpu.VMEM((2 * chips, tokens, width), BF16),
            pltpu.VMEM((tokens, 2 * chips * width), BF16),
            pltpu.VMEM((w.shape[0], 2 * LANES, n), BF16),
            pltpu.SemaphoreType.DMA,
        ],
        compiler_params=pltpu.CompilerParams(vmem_limit_bytes=12 * 1024 * 1024),
        cost_estimate=pl.CostEstimate(
            flops=4 * tokens * n * 2 * chips * width, bytes_accessed=8 * n * chips * width, transcendentals=2 * tokens * n
        ),
        name="branch",
    )(where, same, other, vec, pltpu.with_memory_space_constraint(w, pltpu.HBM))


def mix_body(place_ref, left_ref, right_ref, stat_ref, vec_ref, spatial_ref, w_hbm, keep_ref, give_ref, gated, w, sem, *, offsets, channels):
    gain_at, bias_at = offsets
    tokens, n = left_ref.shape
    groups, span, _ = spatial_ref.shape
    each = n // groups
    copy = pltpu.make_async_copy(w_hbm.at[:, pl.ds(2 * LANES, w.shape[1]), :], w, sem)
    copy.start()
    lines = jnp.concatenate([stat_ref[...], jnp.zeros((LANES - stat_ref.shape[0], tokens), F32)]).T
    mean = lines[:, 0:1] / channels
    inverse = lax.rsqrt(lines[:, 1:2] / channels - mean * mean + EPS)
    centred = ((right_ref[...] - mean) * inverse * vec_ref[:, gain_at : gain_at + n]).astype(BF16)
    target = lax.broadcasted_iota(jnp.int32, (span, span), 0)
    source = lax.broadcasted_iota(jnp.int32, (span, span), 1)
    for g in range(groups):
        causal = jnp.where(source <= target, spatial_ref[g].astype(F32), 0.0).astype(BF16)
        bias = jnp.broadcast_to(vec_ref[:, bias_at + g * span : bias_at + (g + 1) * span], (LANES, span)).T[:, 0:1]
        for b in range(tokens // span):
            at, to = b * span, g * each
            mixed = nn(causal, centred[at : at + span, to : to + each]) + bias
            gated[at : at + span, to : to + each] = (left_ref[at : at + span, to : to + each] * mixed).astype(BF16)
    copy.wait()
    emit(place_ref[1], gated[...], w, 0, n, n, keep_ref, give_ref)


def mix(where, left, right, stat, vec, offsets, spatial, w, rows, shape):
    tokens, n = left.shape
    out = jax.ShapeDtypeStruct(shape, BF16)
    return pl.pallas_call(
        functools.partial(mix_body, offsets=offsets, channels=n * 2 * shape[0]),
        out_shape=(out, out),
        in_specs=[SMEM] + [VMEM] * 5 + [HBM],
        out_specs=(VMEM, VMEM),
        scratch_shapes=[
            pltpu.VMEM((tokens, n), BF16),
            pltpu.VMEM((w.shape[0], rows - 2 * LANES, LANES), BF16),
            pltpu.SemaphoreType.DMA,
        ],
        compiler_params=pltpu.CompilerParams(vmem_limit_bytes=12 * 1024 * 1024),
        cost_estimate=pl.CostEstimate(
            flops=4 * tokens * n * shape[0] * shape[2], bytes_accessed=4 * n * shape[0] * shape[2], transcendentals=0
        ),
        name="mix",
    )(where, left, right, stat, vec, spatial, pltpu.with_memory_space_constraint(w, pltpu.HBM))


def sum_tp(stat):
    stat = stat + swap_cores(stat)
    return (stat + rotate(stat, "tp", 4)) + (rotate(stat, "tp", 2) + rotate(stat, "tp", -2))


def in_a_row(vectors):
    padded = [jnp.pad(v, (0, -v.shape[0] % LANES)) for v in vectors]
    starts = [sum(p.shape[0] for p in padded[:k]) for k in range(len(padded))]
    return jnp.concatenate(padded)[None], starts


def local(
    stream,
    first_gain,
    first_gate,
    first_gate_scale,
    first_up,
    first_up_scale,
    first_down,
    first_down_scale,
    mixer_gain,
    mixer_left,
    mixer_left_scale,
    mixer_right,
    mixer_right_scale,
    channel_gain,
    spatial,
    spatial_bias,
    mixer_out,
    mixer_out_scale,
    second_gain,
    second_gate,
    second_gate_scale,
    second_up,
    second_up_scale,
    second_down,
    second_down_scale,
):
    tp = lax.axis_index("tp").astype(jnp.uint32)
    spots = [tp // 2, tp % 2, lax.axis_index("fs"), lax.axis_index("grp").astype(jnp.uint32) % 2]
    where = jnp.stack([i.astype(jnp.int32) for i in spots])
    hidden = first_gate.shape[1]
    n = mixer_left.shape[1]
    branch_rows = 2 * LANES + n + 16
    shard, stream_rows, two, half = pack_first(
        where,
        mixer_left,
        mixer_right,
        mixer_out,
        mixer_out_scale,
        first_gate.T,
        first_up.T,
        first_down,
        first_down_scale,
    )
    one = ring(shard, stream_rows, half)
    two = lax.all_gather(two, "fs")
    three = lax.all_gather(pack_second(second_gate.T, second_up.T, second_down, second_down_scale), "fs")
    vec, at = in_a_row(
        [
            first_gain,
            first_gate_scale,
            first_up_scale,
            mixer_gain,
            mixer_left_scale,
            mixer_right_scale,
            channel_gain,
            spatial_bias.reshape(-1),
            second_gain,
            second_gate_scale,
            second_up_scale,
        ]
    )

    rest = stream.T
    same, other = gather_tp(rest)
    keep, give = feed(where, same, other, vec, at[0:3], hidden, two, branch_rows, one)
    rest = (rest.astype(F32) + 0.5 * scatter_tp(keep, give)).astype(BF16)

    same, other = gather_tp(rest)
    left, right, stat = branch(where, same, other, vec, at[3:6], n, two)
    keep, give = mix(where, left, right, sum_tp(stat), vec, at[6:8], spatial, two, branch_rows, same.shape)
    rest = (rest.astype(F32) + scatter_tp(keep, give)).astype(BF16)

    same, other = gather_tp(rest)
    keep, give = feed(where, same, other, vec, at[8:11], hidden, three, 0)
    return (rest.astype(F32) + 0.5 * scatter_tp(keep, give)).astype(BF16).T


def solution(mesh):
    return jax.shard_map(
        local,
        mesh=mesh,
        in_specs=(
            P("tp", ("grp", "fs")),
            P(),
            P("fs", "tp"),
            P("tp"),
            P("fs", "tp"),
            P("tp"),
            P("tp", "fs"),
            P("fs"),
            P(),
            P("fs", "tp"),
            P("tp"),
            P("fs", "tp"),
            P("tp"),
            P("tp"),
            P("tp", None, None),
            P("tp", None),
            P("tp", "fs"),
            P("fs"),
            P(),
            P("fs", "tp"),
            P("tp"),
            P("fs", "tp"),
            P("tp"),
            P("tp", "fs"),
            P("fs"),
        ),
        out_specs=P("tp", ("grp", "fs")),
        check_vma=False,
    )
```

```python
import functools

import jax
import jax.numpy as jnp
from jax import lax
from jax.experimental import pallas as pl
from jax.experimental.pallas import tpu as pltpu
from jax.sharding import PartitionSpec as P

EPS = 1e-06
F32 = jnp.float32
BF16 = jnp.bfloat16
LANES = 128
VMEM = pl.BlockSpec(memory_space=pltpu.VMEM)
SMEM = pl.BlockSpec(memory_space=pltpu.SMEM)
HBM = pl.BlockSpec(memory_space=pltpu.HBM)


def rotate(value, axis, by):
    size = lax.axis_size(axis)
    return lax.ppermute(value, axis, [(i, (i + by) % size) for i in range(size)])


def swap_cores(value):
    return lax.ppermute(value, "tp", [(i, i ^ 1) for i in range(lax.axis_size("tp"))])


def ahead(me, by, size):
    return lax.rem(me + jnp.uint32(by % size), jnp.uint32(size))


def swap_groups(value):
    return lax.ppermute(value, "grp", [(i, i ^ 1) for i in range(lax.axis_size("grp"))])


def ring(shard, stream, half):
    size = lax.axis_size("fs")
    pieces = [shard]
    up = down = stream
    for _ in range(1, size // 2):
        up = rotate(up, "fs", 1)
        down = rotate(down, "fs", -1)
        pieces += [up, down, swap_groups(jnp.stack([up[:half], down[:half]]))]
    cut = stream.shape[0] // 32 * 16
    far = jnp.concatenate([rotate(up[:cut], "fs", 1), rotate(down[cut:], "fs", -1)])
    return [*pieces, far, swap_groups(far[None, :half])]


def gather_tp(mine):
    back = rotate(mine, "tp", 2)
    front = rotate(mine, "tp", -2)
    far = rotate(mine, "tp", 4)
    same = jnp.stack([mine, front, far, back])
    return same, swap_cores(same)


def scatter_tp(keep, give):
    chips = keep.shape[0]
    here = lax.axis_index("tp").astype(jnp.uint32) // 2
    both = keep.astype(F32) + swap_cores(give).astype(F32)

    def block(d):
        return lax.dynamic_index_in_dim(both, ahead(here, d, chips), 0, keepdims=False).astype(BF16)

    own = lax.dynamic_index_in_dim(both, here, 0, keepdims=False)
    a = rotate(block(1), "tp", 2)
    b = rotate(block(3), "tp", -2)
    c = rotate(block(2), "tp", 4)
    return own + a.astype(F32) + b.astype(F32) + c.astype(F32)


def put(ref, row, parts):
    for (part, copy), rows in parts:
        copy.wait()
        v = part[...]
        if v.shape[0] == 1:
            hi = v.astype(BF16)
            mid = (v - hi.astype(F32)).astype(BF16)
            low = (v - hi.astype(F32) - mid.astype(F32)).astype(BF16)
            line = lax.broadcasted_iota(jnp.int32, (rows, LANES), 0)
            hi, mid, low = (jnp.broadcast_to(t.astype(F32), (rows, LANES)) for t in (hi, mid, low))
            v = jnp.where(line == 0, hi, jnp.where(line == 1, mid, jnp.where(line == 2, low, 0.0)))
        ref[row : row + rows, :] = v.astype(BF16)
        row += rows


def fetch(sources, buffers, sems):
    copies = [pltpu.make_async_copy(a, b, sems.at[k]) for k, (a, b) in enumerate(zip(sources, buffers))]
    for c in copies:
        c.start()
    return list(zip(buffers, copies))


def pack_first_body(place_ref, *refs, half):
    shard_ref, stream_ref, two_ref = refs[8:11]
    left, right, out, out_scale, gate, up, down, down_scale = fetch(refs[:8], refs[11:19], refs[19])
    put(two_ref, 0, [(left, LANES), (right, LANES), (out, out[0].shape[0]), (out_scale, 16), (gate, gate[0].shape[0])])
    put(shard_ref, 0, [(up, up[0].shape[0]), (down, down[0].shape[0]), (down_scale, 32)])
    odd = place_ref[3]
    stream_ref[:half] = jnp.where(odd == 0, shard_ref[:half], shard_ref[half : 2 * half])
    stream_ref[half:] = shard_ref[2 * half :]


def pack_first(where, left, right, out, out_scale, gate, up, down, down_scale):
    rows = up.shape[0] + down.shape[0] + 32
    half = rows * 7 // 256 * 16
    two_rows = 2 * LANES + out.shape[0] + 16 + gate.shape[0]
    shapes = [jax.ShapeDtypeStruct((n, LANES), BF16) for n in (rows, rows - half, two_rows)]
    sources = [left, right, out, out_scale[None], gate, up, down, down_scale[None]]
    packed = pl.pallas_call(
        functools.partial(pack_first_body, half=half),
        out_shape=shapes,
        in_specs=[SMEM] + [HBM] * len(sources),
        out_specs=[VMEM] * 3,
        scratch_shapes=[pltpu.VMEM(a.shape, F32) for a in sources] + [pltpu.SemaphoreType.DMA((len(sources),))],
        compiler_params=pltpu.CompilerParams(vmem_limit_bytes=8 * 1024 * 1024),
        name="pack_first",
    )(where, *in_hbm(sources))
    return (*packed, half)


def pack_second_body(*refs):
    gate, up, down, down_scale = fetch(refs[:4], refs[5:9], refs[9])
    put(refs[4], 0, [(gate, gate[0].shape[0]), (up, up[0].shape[0]), (down, down[0].shape[0]), (down_scale, 16)])


def pack_second(gate, up, down, down_scale):
    rows = gate.shape[0] + up.shape[0] + down.shape[0] + 16
    sources = [gate, up, down, down_scale[None]]
    return pl.pallas_call(
        pack_second_body,
        out_shape=jax.ShapeDtypeStruct((rows, LANES), BF16),
        in_specs=[HBM] * len(sources),
        out_specs=VMEM,
        scratch_shapes=[pltpu.VMEM(a.shape, F32) for a in sources] + [pltpu.SemaphoreType.DMA((len(sources),))],
        compiler_params=pltpu.CompilerParams(vmem_limit_bytes=8 * 1024 * 1024),
        name="pack_second",
    )(*in_hbm(sources))


def nt(a, b):
    return lax.dot_general(a, b, (((1,), (1,)), ((), ())), preferred_element_type=F32)


def nn(a, b):
    return lax.dot_general(a, b, (((1,), (0,)), ((), ())), preferred_element_type=F32)


def chunks_of(n, step=256):
    return [(at, min(step, n - at)) for at in range(0, n, step)]


def normalise(place_ref, same_ref, other_ref, vec_ref, at, raw, xn):
    chips, tokens, width = same_ref.shape
    here, core = place_ref[0], place_ref[1]
    for d in range(chips):
        chip = (here + d) % chips
        raw[2 * chip + core] = same_ref[d]
        raw[2 * chip + 1 - core] = other_ref[d]
    total = jnp.zeros((tokens, 1), F32)
    for j in range(2 * chips):
        v = raw[j].astype(F32)
        total = total + jnp.sum(v * v, axis=1, keepdims=True)
    inverse = lax.rsqrt(total / (2 * chips * width) + EPS)
    for j in range(2 * chips):
        v = raw[j].astype(F32)
        xn[:, j * width : (j + 1) * width] = (v * inverse * vec_ref[:, at + j * width : at + (j + 1) * width]).astype(BF16)


def lanes(ref, row, n, first, count):
    return jnp.concatenate([ref[f, row : row + n, :] for f in range(first, first + count)], axis=1)


def emit(core, hid, w, row, hidden, scale_row, keep_ref, give_ref):
    per = keep_ref.shape[2] // LANES
    for k in range(keep_ref.shape[0]):
        pair = []
        for c in range(2):
            f = (2 * k + c) * per
            s = lanes(w, scale_row, 16, f, per).astype(F32)
            s = jnp.sum(s, axis=0, keepdims=True)
            pair.append((nn(hid, lanes(w, row, hidden, f, per)) * s).astype(BF16))
        keep_ref[k] = jnp.where(core == 0, pair[0], pair[1])
        give_ref[k] = jnp.where(core == 0, pair[1], pair[0])


def piece_copies(place_ref, pieces, w, row, sems):
    count, rows, _ = w.shape
    me, odd = place_ref[2], place_ref[3]
    half = pieces[3].shape[1]
    ours_at = pl.multiple_of(row + odd * half, 16)
    theirs_at = pl.multiple_of(row + (1 - odd) * half, 16)
    moves = [(pieces[0], w.at[me, pl.ds(row, rows - row)])]
    for step in range(1, count // 2 + 1):
        here = pieces[3 * step - 2 : 3 * step + 1]
        for k, ours in enumerate(here[:-1]):
            f = (me + (count - step if k == 0 else step)) % count
            moves.append((ours.at[pl.ds(0, half)], w.at[f, pl.ds(ours_at, half)]))
            moves.append((here[-1].at[k], w.at[f, pl.ds(theirs_at, half)]))
            moves.append((ours.at[pl.ds(half, ours.shape[0] - half)], w.at[f, pl.ds(row + 2 * half, rows - row - 2 * half)]))
    return [pltpu.make_async_copy(a, b, sems.at[k]) for k, (a, b) in enumerate(moves)]


def feed_body(*refs, hidden, offsets, gate_row, ring_pieces):
    place_ref, same_ref, other_ref, vec_ref, w_hbm = refs[:5]
    pieces = refs[5 : 5 + ring_pieces]
    keep_ref, give_ref, w, raw, xn, hid, sems, piece_sems = refs[5 + ring_pieces :]
    gain_at, gate_at, up_at = offsets
    count, rows, _ = w.shape

    def copy(k, at, n):
        return pltpu.make_async_copy(w_hbm.at[:, pl.ds(gate_row + at, n), :], w.at[:, pl.ds(at, n), :], sems.at[k])

    gates = [copy(k, at, n) for k, (at, n) in enumerate(chunks_of(hidden))]
    if ring_pieces:
        late = piece_copies(place_ref, pieces, w, hidden, piece_sems)
        ups, downs = [late] + [[]] * (len(gates) - 1), []
    else:
        ups = [[copy(len(gates) + k, hidden + at, n)] for k, (at, n) in enumerate(chunks_of(hidden))]
        downs = [copy(2 * len(gates), 2 * hidden, rows - 2 * hidden)]
    for g, u in zip(gates, ups):
        g.start()
        for c in u:
            c.start()
    for c in downs:
        c.start()
    normalise(place_ref, same_ref, other_ref, vec_ref, gain_at, raw, xn)
    x = xn[...]
    for (at, n), gate, up in zip(chunks_of(hidden), gates, ups):
        gate.wait()
        g = nt(x, lanes(w, at, n, 0, count)) * vec_ref[:, gate_at + at : gate_at + at + n]
        for c in up:
            c.wait()
        u = nt(x, lanes(w, hidden + at, n, 0, count)) * vec_ref[:, up_at + at : up_at + at + n]
        hid[:, at : at + n] = (g / (1.0 + jnp.exp(-g)) * u).astype(BF16)
    for c in downs:
        c.wait()
    emit(place_ref[1], hid[...], w, 2 * hidden, hidden, 3 * hidden, keep_ref, give_ref)


def in_hbm(arrays):
    return [pltpu.with_memory_space_constraint(a, pltpu.HBM) for a in arrays]


def feed(where, same, other, vec, offsets, hidden, w, gate_row, pieces=()):
    chips, tokens, width = same.shape
    wide = 2 * chips * width
    rows = hidden + pieces[0].shape[0] if pieces else w.shape[1]
    out = jax.ShapeDtypeStruct(same.shape, BF16)
    return pl.pallas_call(
        functools.partial(feed_body, hidden=hidden, offsets=offsets, gate_row=gate_row, ring_pieces=len(pieces)),
        out_shape=(out, out),
        in_specs=[SMEM, VMEM, VMEM, VMEM, HBM] + [HBM] * len(pieces),
        out_specs=(VMEM, VMEM),
        scratch_shapes=[
            pltpu.VMEM((w.shape[0], rows, LANES), BF16),
            pltpu.VMEM((2 * chips, tokens, width), BF16),
            pltpu.VMEM((tokens, wide), BF16),
            pltpu.VMEM((tokens, hidden), BF16),
            pltpu.SemaphoreType.DMA((2 * len(chunks_of(hidden)) + 1,)),
            pltpu.SemaphoreType.DMA((3 * w.shape[0],)),
        ],
        compiler_params=pltpu.CompilerParams(vmem_limit_bytes=20 * 1024 * 1024),
        cost_estimate=pl.CostEstimate(
            flops=6 * tokens * hidden * wide, bytes_accessed=2 * w.shape[0] * rows * LANES, transcendentals=tokens * hidden
        ),
        name="feed",
    )(where, same, other, vec, *in_hbm([w, *pieces]))


def gelu(t):
    return 0.5 * t * (1.0 + jnp.tanh(0.7978845608028654 * (t + 0.044715 * t * t * t)))


def branch_body(place_ref, same_ref, other_ref, vec_ref, w_hbm, left_ref, right_ref, stat_ref, raw, xn, w, sem, *, offsets):
    gain_at, left_at, right_at = offsets
    n = left_ref.shape[1]
    copy = pltpu.make_async_copy(w_hbm.at[:, pl.ds(0, 2 * LANES), :], w, sem)
    copy.start()
    normalise(place_ref, same_ref, other_ref, vec_ref, gain_at, raw, xn)
    copy.wait()
    wide = w.shape[0] * LANES
    sides = [w[:, at : at + LANES, :].reshape(wide, n) for at in (0, LANES)]
    both = nn(xn[...], jnp.concatenate(sides, axis=1))
    left_ref[...] = gelu(both[:, :n] * vec_ref[:, left_at : left_at + n])
    right = gelu(both[:, n:] * vec_ref[:, right_at : right_at + n])
    right_ref[...] = right
    sums = jnp.sum(right, axis=1, keepdims=True)
    squares = jnp.sum(right * right, axis=1, keepdims=True)
    column = lax.broadcasted_iota(jnp.int32, right.shape, 1)
    stat_ref[...] = jnp.where(column == 0, sums, squares).T[: stat_ref.shape[0]]


def branch(where, same, other, vec, offsets, n, w):
    chips, tokens, width = same.shape
    part = jax.ShapeDtypeStruct((tokens, n), F32)
    return pl.pallas_call(
        functools.partial(branch_body, offsets=offsets),
        out_shape=(part, part, jax.ShapeDtypeStruct((8, tokens), F32)),
        in_specs=[SMEM, VMEM, VMEM, VMEM, HBM],
        out_specs=(VMEM, VMEM, VMEM),
        scratch_shapes=[
            pltpu.VMEM((2 * chips, tokens, width), BF16),
            pltpu.VMEM((tokens, 2 * chips * width), BF16),
            pltpu.VMEM((w.shape[0], 2 * LANES, n), BF16),
            pltpu.SemaphoreType.DMA,
        ],
        compiler_params=pltpu.CompilerParams(vmem_limit_bytes=12 * 1024 * 1024),
        cost_estimate=pl.CostEstimate(
            flops=4 * tokens * n * 2 * chips * width, bytes_accessed=8 * n * chips * width, transcendentals=2 * tokens * n
        ),
        name="branch",
    )(where, same, other, vec, pltpu.with_memory_space_constraint(w, pltpu.HBM))


def mix_body(place_ref, left_ref, right_ref, stat_ref, vec_ref, spatial_ref, w_hbm, keep_ref, give_ref, gated, w, sem, *, offsets, channels):
    gain_at, bias_at = offsets
    tokens, n = left_ref.shape
    groups, span, _ = spatial_ref.shape
    each = n // groups
    copy = pltpu.make_async_copy(w_hbm.at[:, pl.ds(2 * LANES, w.shape[1]), :], w, sem)
    copy.start()
    lines = jnp.concatenate([stat_ref[...], jnp.zeros((LANES - stat_ref.shape[0], tokens), F32)]).T
    mean = lines[:, 0:1] / channels
    inverse = lax.rsqrt(lines[:, 1:2] / channels - mean * mean + EPS)
    centred = ((right_ref[...] - mean) * inverse * vec_ref[:, gain_at : gain_at + n]).astype(BF16)
    target = lax.broadcasted_iota(jnp.int32, (span, span), 0)
    source = lax.broadcasted_iota(jnp.int32, (span, span), 1)
    for g in range(groups):
        causal = jnp.where(source <= target, spatial_ref[g].astype(F32), 0.0).astype(BF16)
        bias = jnp.broadcast_to(vec_ref[:, bias_at + g * span : bias_at + (g + 1) * span], (LANES, span)).T[:, 0:1]
        for b in range(tokens // span):
            at, to = b * span, g * each
            mixed = nn(causal, centred[at : at + span, to : to + each]) + bias
            gated[at : at + span, to : to + each] = (left_ref[at : at + span, to : to + each] * mixed).astype(BF16)
    copy.wait()
    emit(place_ref[1], gated[...], w, 0, n, n, keep_ref, give_ref)


def mix(where, left, right, stat, vec, offsets, spatial, w, rows, shape):
    tokens, n = left.shape
    out = jax.ShapeDtypeStruct(shape, BF16)
    return pl.pallas_call(
        functools.partial(mix_body, offsets=offsets, channels=n * 2 * shape[0]),
        out_shape=(out, out),
        in_specs=[SMEM] + [VMEM] * 5 + [HBM],
        out_specs=(VMEM, VMEM),
        scratch_shapes=[
            pltpu.VMEM((tokens, n), BF16),
            pltpu.VMEM((w.shape[0], rows - 2 * LANES, LANES), BF16),
            pltpu.SemaphoreType.DMA,
        ],
        compiler_params=pltpu.CompilerParams(vmem_limit_bytes=12 * 1024 * 1024),
        cost_estimate=pl.CostEstimate(
            flops=4 * tokens * n * shape[0] * shape[2], bytes_accessed=4 * n * shape[0] * shape[2], transcendentals=0
        ),
        name="mix",
    )(where, left, right, stat, vec, spatial, pltpu.with_memory_space_constraint(w, pltpu.HBM))


def sum_tp(stat):
    stat = stat + swap_cores(stat)
    return (stat + rotate(stat, "tp", 4)) + (rotate(stat, "tp", 2) + rotate(stat, "tp", -2))


def in_a_row(vectors):
    padded = [jnp.pad(v, (0, -v.shape[0] % LANES)) for v in vectors]
    starts = [sum(p.shape[0] for p in padded[:k]) for k in range(len(padded))]
    return jnp.concatenate(padded)[None], starts


def local(
    stream,
    first_gain,
    first_gate,
    first_gate_scale,
    first_up,
    first_up_scale,
    first_down,
    first_down_scale,
    mixer_gain,
    mixer_left,
    mixer_left_scale,
    mixer_right,
    mixer_right_scale,
    channel_gain,
    spatial,
    spatial_bias,
    mixer_out,
    mixer_out_scale,
    second_gain,
    second_gate,
    second_gate_scale,
    second_up,
    second_up_scale,
    second_down,
    second_down_scale,
):
    tp = lax.axis_index("tp").astype(jnp.uint32)
    spots = [tp // 2, tp % 2, lax.axis_index("fs"), lax.axis_index("grp").astype(jnp.uint32) % 2]
    where = jnp.stack([i.astype(jnp.int32) for i in spots])
    hidden = first_gate.shape[1]
    n = mixer_left.shape[1]
    branch_rows = 2 * LANES + n + 16
    shard, stream_rows, two, half = pack_first(
        where,
        mixer_left,
        mixer_right,
        mixer_out,
        mixer_out_scale,
        first_gate.T,
        first_up.T,
        first_down,
        first_down_scale,
    )
    one = ring(shard, stream_rows, half)
    two = lax.all_gather(two, "fs")
    three = lax.all_gather(pack_second(second_gate.T, second_up.T, second_down, second_down_scale), "fs")
    vec, at = in_a_row(
        [
            first_gain,
            first_gate_scale,
            first_up_scale,
            mixer_gain,
            mixer_left_scale,
            mixer_right_scale,
            channel_gain,
            spatial_bias.reshape(-1),
            second_gain,
            second_gate_scale,
            second_up_scale,
        ]
    )

    rest = stream.T
    same, other = gather_tp(rest)
    keep, give = feed(where, same, other, vec, at[0:3], hidden, two, branch_rows, one)
    rest = (rest.astype(F32) + 0.5 * scatter_tp(keep, give)).astype(BF16)

    same, other = gather_tp(rest)
    left, right, stat = branch(where, same, other, vec, at[3:6], n, two)
    keep, give = mix(where, left, right, sum_tp(stat), vec, at[6:8], spatial, two, branch_rows, same.shape)
    rest = (rest.astype(F32) + scatter_tp(keep, give)).astype(BF16)

    same, other = gather_tp(rest)
    keep, give = feed(where, same, other, vec, at[8:11], hidden, three, 0)
    return (rest.astype(F32) + 0.5 * scatter_tp(keep, give)).astype(BF16).T


def solution(mesh):
    return jax.shard_map(
        local,
        mesh=mesh,
        in_specs=(
            P("tp", ("grp", "fs")),
            P(),
            P("fs", "tp"),
            P("tp"),
            P("fs", "tp"),
            P("tp"),
            P("tp", "fs"),
            P("fs"),
            P(),
            P("fs", "tp"),
            P("tp"),
            P("fs", "tp"),
            P("tp"),
            P("tp"),
            P("tp", None, None),
            P("tp", None),
            P("tp", "fs"),
            P("fs"),
            P(),
            P("fs", "tp"),
            P("tp"),
            P("fs", "tp"),
            P("tp"),
            P("tp", "fs"),
            P("fs"),
        ),
        out_specs=P("tp", ("grp", "fs")),
        check_vma=False,
    )
```

```python
import functools

import jax
import jax.numpy as jnp
from jax import lax
from jax.experimental import pallas as pl
from jax.experimental.pallas import tpu as pltpu
from jax.sharding import PartitionSpec as P

EPS = 1e-06
F32 = jnp.float32
BF16 = jnp.bfloat16
LANES = 128
VMEM = pl.BlockSpec(memory_space=pltpu.VMEM)
SMEM = pl.BlockSpec(memory_space=pltpu.SMEM)
HBM = pl.BlockSpec(memory_space=pltpu.HBM)


def rotate(value, axis, by):
    size = lax.axis_size(axis)
    return lax.ppermute(value, axis, [(i, (i + by) % size) for i in range(size)])


def swap_cores(value):
    return lax.ppermute(value, "tp", [(i, i ^ 1) for i in range(lax.axis_size("tp"))])


def ahead(me, by, size):
    return lax.rem(me + jnp.uint32(by % size), jnp.uint32(size))


def swap_groups(value):
    return lax.ppermute(value, "grp", [(i, i ^ 1) for i in range(lax.axis_size("grp"))])


def ring(shard, half, rest):
    size = lax.axis_size("fs")
    pieces = [shard]
    ups, downs = [half, rest], [half, rest]
    for _ in range(1, size // 2):
        ups = [rotate(v, "fs", 1) for v in ups]
        downs = [rotate(v, "fs", -1) for v in downs]
        pieces += [*ups, *downs, swap_groups(jnp.stack([ups[0], downs[0]]))]
    far = []
    for up, down in zip(ups, downs):
        cut = up.shape[0] // 32 * 16
        far.append(jnp.concatenate([rotate(up[:cut], "fs", 1), rotate(down[cut:], "fs", -1)]))
    return [*pieces, *far, swap_groups(far[0][None])]


def gather_tp(mine):
    back = rotate(mine, "tp", 2)
    front = rotate(mine, "tp", -2)
    far = rotate(mine, "tp", 4)
    same = jnp.stack([mine, front, far, back])
    return same, swap_cores(same)


def scatter_tp(keep, give):
    chips = keep.shape[0]
    here = lax.axis_index("tp").astype(jnp.uint32) // 2
    both = keep.astype(F32) + swap_cores(give).astype(F32)

    def block(d):
        return lax.dynamic_index_in_dim(both, ahead(here, d, chips), 0, keepdims=False).astype(BF16)

    own = lax.dynamic_index_in_dim(both, here, 0, keepdims=False)
    a = rotate(block(1), "tp", 2)
    b = rotate(block(3), "tp", -2)
    c = rotate(block(2), "tp", 4)
    return own + a.astype(F32) + b.astype(F32) + c.astype(F32)


def put(ref, row, parts):
    for (part, copy), rows in parts:
        copy.wait()
        v = part[...]
        if v.shape[0] == 1:
            hi = v.astype(BF16)
            mid = (v - hi.astype(F32)).astype(BF16)
            low = (v - hi.astype(F32) - mid.astype(F32)).astype(BF16)
            line = lax.broadcasted_iota(jnp.int32, (rows, LANES), 0)
            hi, mid, low = (jnp.broadcast_to(t.astype(F32), (rows, LANES)) for t in (hi, mid, low))
            v = jnp.where(line == 0, hi, jnp.where(line == 1, mid, jnp.where(line == 2, low, 0.0)))
        ref[row : row + rows, :] = v.astype(BF16)
        row += rows


def fetch(sources, buffers, sems):
    copies = [pltpu.make_async_copy(a, b, sems.at[k]) for k, (a, b) in enumerate(zip(sources, buffers))]
    for c in copies:
        c.start()
    return list(zip(buffers, copies))


def pack_first_body(place_ref, *refs):
    shard_ref, half_ref, rest_ref, two_ref = refs[8:12]
    left, right, out, out_scale, gate, up, down, down_scale = fetch(refs[:8], refs[12:20], refs[20])
    put(two_ref, 0, [(left, LANES), (right, LANES), (out, out[0].shape[0]), (out_scale, 16)])
    half, down_rows = gate[0].shape[0], down[0].shape[0]
    put(shard_ref, 0, [(gate, half), (up, half), (down, down_rows), (down_scale, 32)])
    half_ref[...] = jnp.where(place_ref[3] == 0, shard_ref[:half], shard_ref[half : 2 * half])
    rest_ref[...] = shard_ref[2 * half :]


def pack_first(where, left, right, out, out_scale, gate, up, down, down_scale):
    half, rest = gate.shape[0], down.shape[0] + 32
    rows = [2 * half + rest, half, rest, 2 * LANES + out.shape[0] + 16]
    sources = [left, right, out, out_scale[None], gate, up, down, down_scale[None]]
    return pl.pallas_call(
        pack_first_body,
        out_shape=[jax.ShapeDtypeStruct((n, LANES), BF16) for n in rows],
        in_specs=[SMEM] + [HBM] * len(sources),
        out_specs=[VMEM] * len(rows),
        scratch_shapes=[pltpu.VMEM(a.shape, F32) for a in sources] + [pltpu.SemaphoreType.DMA((len(sources),))],
        compiler_params=pltpu.CompilerParams(vmem_limit_bytes=8 * 1024 * 1024),
        name="pack_first",
    )(where, *in_hbm(sources))


def pack_second_body(*refs):
    gate, up, down, down_scale = fetch(refs[:4], refs[5:9], refs[9])
    put(refs[4], 0, [(gate, gate[0].shape[0]), (up, up[0].shape[0]), (down, down[0].shape[0]), (down_scale, 16)])


def pack_second(gate, up, down, down_scale):
    rows = gate.shape[0] + up.shape[0] + down.shape[0] + 16
    sources = [gate, up, down, down_scale[None]]
    return pl.pallas_call(
        pack_second_body,
        out_shape=jax.ShapeDtypeStruct((rows, LANES), BF16),
        in_specs=[HBM] * len(sources),
        out_specs=VMEM,
        scratch_shapes=[pltpu.VMEM(a.shape, F32) for a in sources] + [pltpu.SemaphoreType.DMA((len(sources),))],
        compiler_params=pltpu.CompilerParams(vmem_limit_bytes=8 * 1024 * 1024),
        name="pack_second",
    )(*in_hbm(sources))


def nt(a, b):
    return lax.dot_general(a, b, (((1,), (1,)), ((), ())), preferred_element_type=F32)


def nn(a, b):
    return lax.dot_general(a, b, (((1,), (0,)), ((), ())), preferred_element_type=F32)


def chunks_of(n, step=256):
    return [(at, min(step, n - at)) for at in range(0, n, step)]


def normalise(place_ref, same_ref, other_ref, vec_ref, at, raw, xn):
    chips, tokens, width = same_ref.shape
    here, core = place_ref[0], place_ref[1]
    for d in range(chips):
        chip = (here + d) % chips
        raw[2 * chip + core] = same_ref[d]
        raw[2 * chip + 1 - core] = other_ref[d]
    total = jnp.zeros((tokens, 1), F32)
    for j in range(2 * chips):
        v = raw[j].astype(F32)
        total = total + jnp.sum(v * v, axis=1, keepdims=True)
    inverse = lax.rsqrt(total / (2 * chips * width) + EPS)
    for j in range(2 * chips):
        v = raw[j].astype(F32)
        xn[:, j * width : (j + 1) * width] = (v * inverse * vec_ref[:, at + j * width : at + (j + 1) * width]).astype(BF16)


def lanes(ref, row, n, first, count):
    return jnp.concatenate([ref[f, row : row + n, :] for f in range(first, first + count)], axis=1)


def emit(core, hid, w, row, hidden, scale_row, keep_ref, give_ref):
    per = keep_ref.shape[2] // LANES
    for k in range(keep_ref.shape[0]):
        pair = []
        for c in range(2):
            f = (2 * k + c) * per
            s = lanes(w, scale_row, 16, f, per).astype(F32)
            s = jnp.sum(s, axis=0, keepdims=True)
            pair.append((nn(hid, lanes(w, row, hidden, f, per)) * s).astype(BF16))
        keep_ref[k] = jnp.where(core == 0, pair[0], pair[1])
        give_ref[k] = jnp.where(core == 0, pair[1], pair[0])


def piece_copies(place_ref, pieces, w, sems):
    count, rows, _ = w.shape
    me, odd = place_ref[2], place_ref[3]
    half = pieces[1].shape[0]
    ours_at = pl.multiple_of(odd * half, 16)
    theirs_at = pl.multiple_of((1 - odd) * half, 16)
    last = pl.ds(2 * half, rows - 2 * half)
    halves = [(pieces[0].at[pl.ds(0, 2 * half)], w.at[me, pl.ds(0, 2 * half)])]
    rests = [(pieces[0].at[last], w.at[me, last])]
    for step in range(1, count // 2 + 1):
        here = pieces[5 * step - 4 : 5 * step + 1]
        for k in range(len(here) // 2):
            f = (me + (count - step if k == 0 else step)) % count
            halves.append((here[2 * k], w.at[f, pl.ds(ours_at, half)]))
            halves.append((here[-1].at[k], w.at[f, pl.ds(theirs_at, half)]))
            rests.append((here[2 * k + 1], w.at[f, last]))
    copies = [pltpu.make_async_copy(a, b, sems.at[k]) for k, (a, b) in enumerate(halves + rests)]
    return copies[: len(halves)], copies[len(halves) :]


def feed_body(*refs, hidden, offsets, parts):
    place_ref, same_ref, other_ref, vec_ref = refs[:4]
    pieces = refs[4 : 4 + parts]
    keep_ref, give_ref, w, raw, xn, hid, sems = refs[4 + parts :]
    gain_at, gate_at, up_at = offsets
    count, rows, _ = w.shape
    chunks = chunks_of(hidden)
    if parts > 1:
        halves, downs = piece_copies(place_ref, pieces, w, sems)
        early = [halves] + [[]] * (len(chunks) - 1)
    else:
        moves = [(row + at, n) for at, n in chunks for row in (0, hidden)] + [(2 * hidden, rows - 2 * hidden)]
        copies = [
            pltpu.make_async_copy(pieces[0].at[:, pl.ds(at, n), :], w.at[:, pl.ds(at, n), :], sems.at[k])
            for k, (at, n) in enumerate(moves)
        ]
        early = [copies[2 * k : 2 * k + 2] for k in range(len(chunks))]
        downs = copies[2 * len(chunks) :]
    for group in [*early, downs]:
        for c in group:
            c.start()
    normalise(place_ref, same_ref, other_ref, vec_ref, gain_at, raw, xn)
    x = xn[...]
    for (at, n), group in zip(chunks, early):
        for c in group:
            c.wait()
        g = nt(x, lanes(w, at, n, 0, count)) * vec_ref[:, gate_at + at : gate_at + at + n]
        u = nt(x, lanes(w, hidden + at, n, 0, count)) * vec_ref[:, up_at + at : up_at + at + n]
        hid[:, at : at + n] = (g / (1.0 + jnp.exp(-g)) * u).astype(BF16)
    for c in downs:
        c.wait()
    emit(place_ref[1], hid[...], w, 2 * hidden, hidden, 3 * hidden, keep_ref, give_ref)


def in_hbm(arrays):
    return [pltpu.with_memory_space_constraint(a, pltpu.HBM) for a in arrays]


def feed(where, same, other, vec, offsets, hidden, pieces, count):
    chips, tokens, width = same.shape
    wide = 2 * chips * width
    rows = pieces[0].shape[-2]
    out = jax.ShapeDtypeStruct(same.shape, BF16)
    return pl.pallas_call(
        functools.partial(feed_body, hidden=hidden, offsets=offsets, parts=len(pieces)),
        out_shape=(out, out),
        in_specs=[SMEM, VMEM, VMEM, VMEM] + [HBM] * len(pieces),
        out_specs=(VMEM, VMEM),
        scratch_shapes=[
            pltpu.VMEM((count, rows, LANES), BF16),
            pltpu.VMEM((2 * chips, tokens, width), BF16),
            pltpu.VMEM((tokens, wide), BF16),
            pltpu.VMEM((tokens, hidden), BF16),
            pltpu.SemaphoreType.DMA((3 * count,)),
        ],
        compiler_params=pltpu.CompilerParams(vmem_limit_bytes=20 * 1024 * 1024),
        cost_estimate=pl.CostEstimate(
            flops=6 * tokens * hidden * wide, bytes_accessed=2 * count * rows * LANES, transcendentals=tokens * hidden
        ),
        name="feed",
    )(where, same, other, vec, *in_hbm(pieces))


def gelu(t):
    return 0.5 * t * (1.0 + jnp.tanh(0.7978845608028654 * (t + 0.044715 * t * t * t)))


def branch_body(place_ref, same_ref, other_ref, vec_ref, w_hbm, left_ref, right_ref, stat_ref, raw, xn, w, sem, *, offsets):
    gain_at, left_at, right_at = offsets
    n = left_ref.shape[1]
    copy = pltpu.make_async_copy(w_hbm.at[:, pl.ds(0, 2 * LANES), :], w, sem)
    copy.start()
    normalise(place_ref, same_ref, other_ref, vec_ref, gain_at, raw, xn)
    copy.wait()
    wide = w.shape[0] * LANES
    sides = [w[:, at : at + LANES, :].reshape(wide, n) for at in (0, LANES)]
    both = nn(xn[...], jnp.concatenate(sides, axis=1))
    left_ref[...] = gelu(both[:, :n] * vec_ref[:, left_at : left_at + n])
    right = gelu(both[:, n:] * vec_ref[:, right_at : right_at + n])
    right_ref[...] = right
    sums = jnp.sum(right, axis=1, keepdims=True)
    squares = jnp.sum(right * right, axis=1, keepdims=True)
    column = lax.broadcasted_iota(jnp.int32, right.shape, 1)
    stat_ref[...] = jnp.where(column == 0, sums, squares).T[: stat_ref.shape[0]]


def branch(where, same, other, vec, offsets, n, w):
    chips, tokens, width = same.shape
    part = jax.ShapeDtypeStruct((tokens, n), F32)
    return pl.pallas_call(
        functools.partial(branch_body, offsets=offsets),
        out_shape=(part, part, jax.ShapeDtypeStruct((8, tokens), F32)),
        in_specs=[SMEM, VMEM, VMEM, VMEM, HBM],
        out_specs=(VMEM, VMEM, VMEM),
        scratch_shapes=[
            pltpu.VMEM((2 * chips, tokens, width), BF16),
            pltpu.VMEM((tokens, 2 * chips * width), BF16),
            pltpu.VMEM((w.shape[0], 2 * LANES, n), BF16),
            pltpu.SemaphoreType.DMA,
        ],
        compiler_params=pltpu.CompilerParams(vmem_limit_bytes=12 * 1024 * 1024),
        cost_estimate=pl.CostEstimate(
            flops=4 * tokens * n * 2 * chips * width, bytes_accessed=8 * n * chips * width, transcendentals=2 * tokens * n
        ),
        name="branch",
    )(where, same, other, vec, pltpu.with_memory_space_constraint(w, pltpu.HBM))


def mix_body(place_ref, left_ref, right_ref, stat_ref, vec_ref, spatial_ref, w_hbm, keep_ref, give_ref, gated, w, sem, *, offsets, channels):
    gain_at, bias_at = offsets
    tokens, n = left_ref.shape
    groups, span, _ = spatial_ref.shape
    each = n // groups
    copy = pltpu.make_async_copy(w_hbm.at[:, pl.ds(2 * LANES, w.shape[1]), :], w, sem)
    copy.start()
    lines = jnp.concatenate([stat_ref[...], jnp.zeros((LANES - stat_ref.shape[0], tokens), F32)]).T
    mean = lines[:, 0:1] / channels
    inverse = lax.rsqrt(lines[:, 1:2] / channels - mean * mean + EPS)
    centred = ((right_ref[...] - mean) * inverse * vec_ref[:, gain_at : gain_at + n]).astype(BF16)
    target = lax.broadcasted_iota(jnp.int32, (span, span), 0)
    source = lax.broadcasted_iota(jnp.int32, (span, span), 1)
    for g in range(groups):
        causal = jnp.where(source <= target, spatial_ref[g].astype(F32), 0.0).astype(BF16)
        bias = jnp.broadcast_to(vec_ref[:, bias_at + g * span : bias_at + (g + 1) * span], (LANES, span)).T[:, 0:1]
        for b in range(tokens // span):
            at, to = b * span, g * each
            mixed = nn(causal, centred[at : at + span, to : to + each]) + bias
            gated[at : at + span, to : to + each] = (left_ref[at : at + span, to : to + each] * mixed).astype(BF16)
    copy.wait()
    emit(place_ref[1], gated[...], w, 0, n, n, keep_ref, give_ref)


def mix(where, left, right, stat, vec, offsets, spatial, w, rows, shape):
    tokens, n = left.shape
    out = jax.ShapeDtypeStruct(shape, BF16)
    return pl.pallas_call(
        functools.partial(mix_body, offsets=offsets, channels=n * 2 * shape[0]),
        out_shape=(out, out),
        in_specs=[SMEM] + [VMEM] * 5 + [HBM],
        out_specs=(VMEM, VMEM),
        scratch_shapes=[
            pltpu.VMEM((tokens, n), BF16),
            pltpu.VMEM((w.shape[0], rows - 2 * LANES, LANES), BF16),
            pltpu.SemaphoreType.DMA,
        ],
        compiler_params=pltpu.CompilerParams(vmem_limit_bytes=12 * 1024 * 1024),
        cost_estimate=pl.CostEstimate(
            flops=4 * tokens * n * shape[0] * shape[2], bytes_accessed=4 * n * shape[0] * shape[2], transcendentals=0
        ),
        name="mix",
    )(where, left, right, stat, vec, spatial, pltpu.with_memory_space_constraint(w, pltpu.HBM))


def sum_tp(stat):
    stat = stat + swap_cores(stat)
    return (stat + rotate(stat, "tp", 4)) + (rotate(stat, "tp", 2) + rotate(stat, "tp", -2))


def in_a_row(vectors):
    padded = [jnp.pad(v, (0, -v.shape[0] % LANES)) for v in vectors]
    starts = [sum(p.shape[0] for p in padded[:k]) for k in range(len(padded))]
    return jnp.concatenate(padded)[None], starts


def local(
    stream,
    first_gain,
    first_gate,
    first_gate_scale,
    first_up,
    first_up_scale,
    first_down,
    first_down_scale,
    mixer_gain,
    mixer_left,
    mixer_left_scale,
    mixer_right,
    mixer_right_scale,
    channel_gain,
    spatial,
    spatial_bias,
    mixer_out,
    mixer_out_scale,
    second_gain,
    second_gate,
    second_gate_scale,
    second_up,
    second_up_scale,
    second_down,
    second_down_scale,
):
    tp = lax.axis_index("tp").astype(jnp.uint32)
    spots = [tp // 2, tp % 2, lax.axis_index("fs"), lax.axis_index("grp").astype(jnp.uint32) % 2]
    where = jnp.stack([i.astype(jnp.int32) for i in spots])
    hidden = first_gate.shape[1]
    n = mixer_left.shape[1]
    branch_rows = 2 * LANES + n + 16
    shard, half, last, two = pack_first(
        where,
        mixer_left,
        mixer_right,
        mixer_out,
        mixer_out_scale,
        first_gate.T,
        first_up.T,
        first_down,
        first_down_scale,
    )
    one = ring(shard, half, last)
    two = lax.all_gather(two, "fs")
    three = lax.all_gather(pack_second(second_gate.T, second_up.T, second_down, second_down_scale), "fs")
    vec, at = in_a_row(
        [
            first_gain,
            first_gate_scale,
            first_up_scale,
            mixer_gain,
            mixer_left_scale,
            mixer_right_scale,
            channel_gain,
            spatial_bias.reshape(-1),
            second_gain,
            second_gate_scale,
            second_up_scale,
        ]
    )

    rest = stream.T
    same, other = gather_tp(rest)
    keep, give = feed(where, same, other, vec, at[0:3], hidden, one, two.shape[0])
    rest = (rest.astype(F32) + 0.5 * scatter_tp(keep, give)).astype(BF16)

    same, other = gather_tp(rest)
    left, right, stat = branch(where, same, other, vec, at[3:6], n, two)
    keep, give = mix(where, left, right, sum_tp(stat), vec, at[6:8], spatial, two, branch_rows, same.shape)
    rest = (rest.astype(F32) + scatter_tp(keep, give)).astype(BF16)

    same, other = gather_tp(rest)
    keep, give = feed(where, same, other, vec, at[8:11], hidden, [three], two.shape[0])
    return (rest.astype(F32) + 0.5 * scatter_tp(keep, give)).astype(BF16).T


def solution(mesh):
    return jax.shard_map(
        local,
        mesh=mesh,
        in_specs=(
            P("tp", ("grp", "fs")),
            P(),
            P("fs", "tp"),
            P("tp"),
            P("fs", "tp"),
            P("tp"),
            P("tp", "fs"),
            P("fs"),
            P(),
            P("fs", "tp"),
            P("tp"),
            P("fs", "tp"),
            P("tp"),
            P("tp"),
            P("tp", None, None),
            P("tp", None),
            P("tp", "fs"),
            P("fs"),
            P(),
            P("fs", "tp"),
            P("tp"),
            P("fs", "tp"),
            P("tp"),
            P("tp", "fs"),
            P("fs"),
        ),
        out_specs=P("tp", ("grp", "fs")),
        check_vma=False,
    )
```

```python
import functools

import jax
import jax.numpy as jnp
from jax import lax
from jax.experimental import pallas as pl
from jax.experimental.pallas import tpu as pltpu
from jax.sharding import PartitionSpec as P


EPS = 1e-06
F32 = jnp.float32
BF16 = jnp.bfloat16
LANES = 128
VMEM = pl.BlockSpec(memory_space=pltpu.VMEM)
SMEM = pl.BlockSpec(memory_space=pltpu.SMEM)
HBM = pl.BlockSpec(memory_space=pltpu.HBM)


def rotate(value, axis, by):
    size = lax.axis_size(axis)
    return lax.ppermute(value, axis, [(i, (i + by) % size) for i in range(size)])


def swap_cores(value):
    return lax.ppermute(value, "tp", [(i, i ^ 1) for i in range(lax.axis_size("tp"))])


def ahead(me, by, size):
    return lax.rem(me + jnp.uint32(by % size), jnp.uint32(size))


def swap_groups(value):
    return lax.ppermute(value, "grp", [(i, i ^ 1) for i in range(lax.axis_size("grp"))])


def step_on(value, by):
    return rotate(value, "fs", by)


def ring(shard, half, rest):
    size = lax.axis_size("fs")
    pieces = [shard]
    ups, downs = [half, rest], [half, rest]
    for _ in range(1, size // 2):
        ups = [step_on(v, 1) for v in ups]
        downs = [step_on(v, -1) for v in downs]
        other = swap_groups(jnp.stack([ups[0], downs[0]]))
        pieces += [*ups, *downs, other]
    far = []
    for up, down in zip(ups, downs):
        cut = up.shape[0] // 32 * 16
        both = [step_on(up[:cut], 1), step_on(down[cut:], -1)]
        far.append(jnp.concatenate(both))
    return [*pieces, *far, swap_groups(far[0][None])]


def gather_tp(mine):
    back = rotate(mine, "tp", 2)
    front = rotate(mine, "tp", -2)
    far = rotate(mine, "tp", 4)
    same = jnp.stack([mine, front, far, back])
    return same, swap_cores(same)


def scatter_tp(keep, give):
    chips = keep.shape[0]
    here = lax.axis_index("tp").astype(jnp.uint32) // 2
    both = keep.astype(F32) + swap_cores(give).astype(F32)

    def block(d):
        return lax.dynamic_index_in_dim(both, ahead(here, d, chips), 0, keepdims=False).astype(BF16)

    own = lax.dynamic_index_in_dim(both, here, 0, keepdims=False)
    a = rotate(block(1), "tp", 2)
    b = rotate(block(3), "tp", -2)
    c = rotate(block(2), "tp", 4)
    return own + a.astype(F32) + b.astype(F32) + c.astype(F32)


def put(ref, row, parts):
    for (part, copy), rows in parts:
        copy.wait()
        v = part[...]
        if v.shape[0] == 1:
            hi = v.astype(BF16)
            mid = (v - hi.astype(F32)).astype(BF16)
            low = (v - hi.astype(F32) - mid.astype(F32)).astype(BF16)
            line = lax.broadcasted_iota(jnp.int32, (rows, LANES), 0)
            hi, mid, low = (jnp.broadcast_to(t.astype(F32), (rows, LANES)) for t in (hi, mid, low))
            v = jnp.where(line == 0, hi, jnp.where(line == 1, mid, jnp.where(line == 2, low, 0.0)))
        ref[row : row + rows, :] = v.astype(BF16)
        row += rows


def fetch(sources, buffers, sems):
    copies = [pltpu.make_async_copy(a, b, sems.at[k]) for k, (a, b) in enumerate(zip(sources, buffers))]
    for c in copies:
        c.start()
    return list(zip(buffers, copies))


def pack_first_body(place_ref, *refs):
    shard_ref, half_ref, rest_ref, two_ref = refs[8:12]
    left, right, out, out_scale, gate, up, down, down_scale = fetch(refs[:8], refs[12:20], refs[20])
    put(two_ref, 0, [(left, LANES), (right, LANES), (out, out[0].shape[0]), (out_scale, 16)])
    half, down_rows = gate[0].shape[0], down[0].shape[0]
    put(shard_ref, 0, [(gate, half), (up, half), (down, down_rows), (down_scale, 32)])
    half_ref[...] = jnp.where(place_ref[3] == 0, shard_ref[:half], shard_ref[half : 2 * half])
    rest_ref[...] = shard_ref[2 * half :]


def pack_first(where, left, right, out, out_scale, gate, up, down, down_scale):
    half, rest = gate.shape[0], down.shape[0] + 32
    rows = [2 * half + rest, half, rest, 2 * LANES + out.shape[0] + 16]
    sources = [left, right, out, out_scale[None], gate, up, down, down_scale[None]]
    return pl.pallas_call(
        pack_first_body,
        out_shape=[jax.ShapeDtypeStruct((n, LANES), BF16) for n in rows],
        in_specs=[SMEM] + [HBM] * len(sources),
        out_specs=[VMEM] * len(rows),
        scratch_shapes=[pltpu.VMEM(a.shape, F32) for a in sources] + [pltpu.SemaphoreType.DMA((len(sources),))],
        compiler_params=pltpu.CompilerParams(vmem_limit_bytes=8 * 1024 * 1024),
        name="pack_first",
    )(where, *in_hbm(sources))


def pack_second_body(*refs):
    gate, up, down, down_scale = fetch(refs[:4], refs[5:9], refs[9])
    put(refs[4], 0, [(gate, gate[0].shape[0]), (up, up[0].shape[0]), (down, down[0].shape[0]), (down_scale, 16)])


def pack_second(gate, up, down, down_scale):
    rows = gate.shape[0] + up.shape[0] + down.shape[0] + 16
    sources = [gate, up, down, down_scale[None]]
    return pl.pallas_call(
        pack_second_body,
        out_shape=jax.ShapeDtypeStruct((rows, LANES), BF16),
        in_specs=[HBM] * len(sources),
        out_specs=VMEM,
        scratch_shapes=[pltpu.VMEM(a.shape, F32) for a in sources] + [pltpu.SemaphoreType.DMA((len(sources),))],
        compiler_params=pltpu.CompilerParams(vmem_limit_bytes=8 * 1024 * 1024),
        name="pack_second",
    )(*in_hbm(sources))


def nt(a, b):
    return lax.dot_general(a, b, (((1,), (1,)), ((), ())), preferred_element_type=F32)


def nn(a, b):
    return lax.dot_general(a, b, (((1,), (0,)), ((), ())), preferred_element_type=F32)


def chunks_of(n, step=256):
    return [(at, min(step, n - at)) for at in range(0, n, step)]


def normalise(place_ref, same_ref, other_ref, vec_ref, at, raw, xn):
    chips, tokens, width = same_ref.shape
    here, core = place_ref[0], place_ref[1]
    for d in range(chips):
        chip = (here + d) % chips
        raw[2 * chip + core] = same_ref[d]
        raw[2 * chip + 1 - core] = other_ref[d]
    total = jnp.zeros((tokens, 1), F32)
    for j in range(2 * chips):
        v = raw[j].astype(F32)
        total = total + jnp.sum(v * v, axis=1, keepdims=True)
    inverse = lax.rsqrt(total / (2 * chips * width) + EPS)
    for j in range(2 * chips):
        v = raw[j].astype(F32)
        xn[:, j * width : (j + 1) * width] = (v * inverse * vec_ref[:, at + j * width : at + (j + 1) * width]).astype(BF16)


def lanes(ref, row, n, first, count):
    return jnp.concatenate([ref[f, row : row + n, :] for f in range(first, first + count)], axis=1)


def emit(core, hid, w, row, hidden, scale_row, keep_ref, give_ref):
    per = keep_ref.shape[2] // LANES
    for k in range(keep_ref.shape[0]):
        pair = []
        for c in range(2):
            f = (2 * k + c) * per
            s = lanes(w, scale_row, 16, f, per).astype(F32)
            s = jnp.sum(s, axis=0, keepdims=True)
            pair.append((nn(hid, lanes(w, row, hidden, f, per)) * s).astype(BF16))
        keep_ref[k] = jnp.where(core == 0, pair[0], pair[1])
        give_ref[k] = jnp.where(core == 0, pair[1], pair[0])


def piece_copies(place_ref, pieces, w, sems):
    count, rows, _ = w.shape
    me, odd = place_ref[2], place_ref[3]
    half = pieces[1].shape[0]
    ours_at = pl.multiple_of(odd * half, 16)
    theirs_at = pl.multiple_of((1 - odd) * half, 16)
    last = pl.ds(2 * half, rows - 2 * half)
    halves = [(pieces[0].at[pl.ds(0, 2 * half)], w.at[me, pl.ds(0, 2 * half)])]
    rests = [(pieces[0].at[last], w.at[me, last])]
    for step in range(1, count // 2 + 1):
        here = pieces[5 * step - 4 : 5 * step + 1]
        for k in range(len(here) // 2):
            f = (me + (count - step if k == 0 else step)) % count
            halves.append((here[2 * k], w.at[f, pl.ds(ours_at, half)]))
            halves.append((here[-1].at[k], w.at[f, pl.ds(theirs_at, half)]))
            rests.append((here[2 * k + 1], w.at[f, last]))
    copies = [pltpu.make_async_copy(a, b, sems.at[k]) for k, (a, b) in enumerate(halves + rests)]
    return copies[: len(halves)], copies[len(halves) :]


def feed_body(*refs, hidden, offsets, parts):
    place_ref, same_ref, other_ref, vec_ref = refs[:4]
    pieces = refs[4 : 4 + parts]
    keep_ref, give_ref, w, raw, xn, hid, sems = refs[4 + parts :]
    gain_at, gate_at, up_at = offsets
    count, rows, _ = w.shape
    chunks = chunks_of(hidden)
    if parts > 1:
        halves, downs = piece_copies(place_ref, pieces, w, sems)
        early = [halves] + [[]] * (len(chunks) - 1)
    else:
        moves = [(row + at, n) for at, n in chunks for row in (0, hidden)] + [(2 * hidden, rows - 2 * hidden)]
        copies = [
            pltpu.make_async_copy(pieces[0].at[:, pl.ds(at, n), :], w.at[:, pl.ds(at, n), :], sems.at[k])
            for k, (at, n) in enumerate(moves)
        ]
        early = [copies[2 * k : 2 * k + 2] for k in range(len(chunks))]
        downs = copies[2 * len(chunks) :]
    for group in [*early, downs]:
        for c in group:
            c.start()
    normalise(place_ref, same_ref, other_ref, vec_ref, gain_at, raw, xn)
    x = xn[...]
    for (at, n), group in zip(chunks, early):
        for c in group:
            c.wait()
        g = nt(x, lanes(w, at, n, 0, count)) * vec_ref[:, gate_at + at : gate_at + at + n]
        u = nt(x, lanes(w, hidden + at, n, 0, count)) * vec_ref[:, up_at + at : up_at + at + n]
        hid[:, at : at + n] = (g / (1.0 + jnp.exp(-g)) * u).astype(BF16)
    for c in downs:
        c.wait()
    emit(place_ref[1], hid[...], w, 2 * hidden, hidden, 3 * hidden, keep_ref, give_ref)


def in_hbm(arrays):
    return [pltpu.with_memory_space_constraint(a, pltpu.HBM) for a in arrays]


def feed(where, same, other, vec, offsets, hidden, pieces, count):
    chips, tokens, width = same.shape
    wide = 2 * chips * width
    rows = pieces[0].shape[-2]
    out = jax.ShapeDtypeStruct(same.shape, BF16)
    return pl.pallas_call(
        functools.partial(feed_body, hidden=hidden, offsets=offsets, parts=len(pieces)),
        out_shape=(out, out),
        in_specs=[SMEM, VMEM, VMEM, VMEM] + [HBM] * len(pieces),
        out_specs=(VMEM, VMEM),
        scratch_shapes=[
            pltpu.VMEM((count, rows, LANES), BF16),
            pltpu.VMEM((2 * chips, tokens, width), BF16),
            pltpu.VMEM((tokens, wide), BF16),
            pltpu.VMEM((tokens, hidden), BF16),
            pltpu.SemaphoreType.DMA((3 * count,)),
        ],
        compiler_params=pltpu.CompilerParams(vmem_limit_bytes=20 * 1024 * 1024),
        cost_estimate=pl.CostEstimate(
            flops=6 * tokens * hidden * wide, bytes_accessed=2 * count * rows * LANES, transcendentals=tokens * hidden
        ),
        name="feed",
    )(where, same, other, vec, *in_hbm(pieces))


def gelu(t):
    return 0.5 * t * (1.0 + jnp.tanh(0.7978845608028654 * (t + 0.044715 * t * t * t)))


def branch_body(place_ref, same_ref, other_ref, vec_ref, w_hbm, left_ref, right_ref, stat_ref, raw, xn, w, sem, *, offsets):
    gain_at, left_at, right_at = offsets
    n = left_ref.shape[1]
    copy = pltpu.make_async_copy(w_hbm.at[:, pl.ds(0, 2 * LANES), :], w, sem)
    copy.start()
    normalise(place_ref, same_ref, other_ref, vec_ref, gain_at, raw, xn)
    copy.wait()
    wide = w.shape[0] * LANES
    sides = [w[:, at : at + LANES, :].reshape(wide, n) for at in (0, LANES)]
    both = nn(xn[...], jnp.concatenate(sides, axis=1))
    left_ref[...] = gelu(both[:, :n] * vec_ref[:, left_at : left_at + n])
    right = gelu(both[:, n:] * vec_ref[:, right_at : right_at + n])
    right_ref[...] = right
    sums = jnp.sum(right, axis=1, keepdims=True)
    squares = jnp.sum(right * right, axis=1, keepdims=True)
    column = lax.broadcasted_iota(jnp.int32, right.shape, 1)
    stat_ref[...] = jnp.where(column == 0, sums, squares).T[: stat_ref.shape[0]]


def branch(where, same, other, vec, offsets, n, w):
    chips, tokens, width = same.shape
    part = jax.ShapeDtypeStruct((tokens, n), F32)
    return pl.pallas_call(
        functools.partial(branch_body, offsets=offsets),
        out_shape=(part, part, jax.ShapeDtypeStruct((8, tokens), F32)),
        in_specs=[SMEM, VMEM, VMEM, VMEM, HBM],
        out_specs=(VMEM, VMEM, VMEM),
        scratch_shapes=[
            pltpu.VMEM((2 * chips, tokens, width), BF16),
            pltpu.VMEM((tokens, 2 * chips * width), BF16),
            pltpu.VMEM((w.shape[0], 2 * LANES, n), BF16),
            pltpu.SemaphoreType.DMA,
        ],
        compiler_params=pltpu.CompilerParams(vmem_limit_bytes=12 * 1024 * 1024),
        cost_estimate=pl.CostEstimate(
            flops=4 * tokens * n * 2 * chips * width, bytes_accessed=8 * n * chips * width, transcendentals=2 * tokens * n
        ),
        name="branch",
    )(where, same, other, vec, pltpu.with_memory_space_constraint(w, pltpu.HBM))


def mix_body(place_ref, left_ref, right_ref, stat_ref, vec_ref, spatial_ref, w_hbm, keep_ref, give_ref, gated, w, sem, *, offsets, channels):
    gain_at, bias_at = offsets
    tokens, n = left_ref.shape
    groups, span, _ = spatial_ref.shape
    each = n // groups
    copy = pltpu.make_async_copy(w_hbm.at[:, pl.ds(2 * LANES, w.shape[1]), :], w, sem)
    copy.start()
    lines = jnp.concatenate([stat_ref[...], jnp.zeros((LANES - stat_ref.shape[0], tokens), F32)]).T
    mean = lines[:, 0:1] / channels
    inverse = lax.rsqrt(lines[:, 1:2] / channels - mean * mean + EPS)
    centred = ((right_ref[...] - mean) * inverse * vec_ref[:, gain_at : gain_at + n]).astype(BF16)
    target = lax.broadcasted_iota(jnp.int32, (span, span), 0)
    source = lax.broadcasted_iota(jnp.int32, (span, span), 1)
    for g in range(groups):
        causal = jnp.where(source <= target, spatial_ref[g].astype(F32), 0.0).astype(BF16)
        bias = jnp.broadcast_to(vec_ref[:, bias_at + g * span : bias_at + (g + 1) * span], (LANES, span)).T[:, 0:1]
        for b in range(tokens // span):
            at, to = b * span, g * each
            mixed = nn(causal, centred[at : at + span, to : to + each]) + bias
            gated[at : at + span, to : to + each] = (left_ref[at : at + span, to : to + each] * mixed).astype(BF16)
    copy.wait()
    emit(place_ref[1], gated[...], w, 0, n, n, keep_ref, give_ref)


def mix(where, left, right, stat, vec, offsets, spatial, w, rows, shape):
    tokens, n = left.shape
    out = jax.ShapeDtypeStruct(shape, BF16)
    return pl.pallas_call(
        functools.partial(mix_body, offsets=offsets, channels=n * 2 * shape[0]),
        out_shape=(out, out),
        in_specs=[SMEM] + [VMEM] * 5 + [HBM],
        out_specs=(VMEM, VMEM),
        scratch_shapes=[
            pltpu.VMEM((tokens, n), BF16),
            pltpu.VMEM((w.shape[0], rows - 2 * LANES, LANES), BF16),
            pltpu.SemaphoreType.DMA,
        ],
        compiler_params=pltpu.CompilerParams(vmem_limit_bytes=12 * 1024 * 1024),
        cost_estimate=pl.CostEstimate(
            flops=4 * tokens * n * shape[0] * shape[2], bytes_accessed=4 * n * shape[0] * shape[2], transcendentals=0
        ),
        name="mix",
    )(where, left, right, stat, vec, spatial, pltpu.with_memory_space_constraint(w, pltpu.HBM))


def sum_tp(stat):
    stat = stat + swap_cores(stat)
    return (stat + rotate(stat, "tp", 4)) + (rotate(stat, "tp", 2) + rotate(stat, "tp", -2))


def in_a_row(vectors):
    padded = [jnp.pad(v, (0, -v.shape[0] % LANES)) for v in vectors]
    starts = [sum(p.shape[0] for p in padded[:k]) for k in range(len(padded))]
    return jnp.concatenate(padded)[None], starts


def layer(
    stream,
    first_gain,
    first_gate,
    first_gate_scale,
    first_up,
    first_up_scale,
    first_down,
    first_down_scale,
    mixer_gain,
    mixer_left,
    mixer_left_scale,
    mixer_right,
    mixer_right_scale,
    channel_gain,
    spatial,
    spatial_bias,
    mixer_out,
    mixer_out_scale,
    second_gain,
    second_gate,
    second_gate_scale,
    second_up,
    second_up_scale,
    second_down,
    second_down_scale,
):
    tp = lax.axis_index("tp").astype(jnp.uint32)
    spots = [tp // 2, tp % 2, lax.axis_index("fs"), lax.axis_index("grp").astype(jnp.uint32) % 2]
    where = jnp.stack([i.astype(jnp.int32) for i in spots])
    hidden = first_gate.shape[1]
    n = mixer_left.shape[1]
    branch_rows = 2 * LANES + n + 16
    shard, half, last, two = pack_first(
        where,
        mixer_left,
        mixer_right,
        mixer_out,
        mixer_out_scale,
        first_gate.T,
        first_up.T,
        first_down,
        first_down_scale,
    )
    one = ring(shard, half, last)
    two = lax.all_gather(two, "fs")
    three = lax.all_gather(pack_second(second_gate.T, second_up.T, second_down, second_down_scale), "fs")
    vec, at = in_a_row(
        [
            first_gain,
            first_gate_scale,
            first_up_scale,
            mixer_gain,
            mixer_left_scale,
            mixer_right_scale,
            channel_gain,
            spatial_bias.reshape(-1),
            second_gain,
            second_gate_scale,
            second_up_scale,
        ]
    )

    rest = stream.T
    same, other = gather_tp(rest)
    keep, give = feed(where, same, other, vec, at[0:3], hidden, one, two.shape[0])
    rest = (rest.astype(F32) + 0.5 * scatter_tp(keep, give)).astype(BF16)

    same, other = gather_tp(rest)
    left, right, stat = branch(where, same, other, vec, at[3:6], n, two)
    keep, give = mix(where, left, right, sum_tp(stat), vec, at[6:8], spatial, two, branch_rows, same.shape)
    rest = (rest.astype(F32) + scatter_tp(keep, give)).astype(BF16)

    same, other = gather_tp(rest)
    keep, give = feed(where, same, other, vec, at[8:11], hidden, [three], two.shape[0])
    return (rest.astype(F32) + 0.5 * scatter_tp(keep, give)).astype(BF16).T


def solution(mesh):
    return jax.shard_map(
        layer,
        mesh=mesh,
        in_specs=(
            P("tp", ("grp", "fs")),
            P(),
            P("fs", "tp"),
            P("tp"),
            P("fs", "tp"),
            P("tp"),
            P("tp", "fs"),
            P("fs"),
            P(),
            P("fs", "tp"),
            P("tp"),
            P("fs", "tp"),
            P("tp"),
            P("tp"),
            P("tp", None, None),
            P("tp", None),
            P("tp", "fs"),
            P("fs"),
            P(),
            P("fs", "tp"),
            P("tp"),
            P("fs", "tp"),
            P("tp"),
            P("tp", "fs"),
            P("fs"),
        ),
        out_specs=P("tp", ("grp", "fs")),
        check_vma=False,
    )
```

```python
import functools

import jax
import jax.numpy as jnp
from jax import lax
from jax.experimental import pallas as pl
from jax.experimental.pallas import tpu as pltpu
from jax.sharding import PartitionSpec as P


EPS = 1e-06
F32 = jnp.float32
BF16 = jnp.bfloat16
LANES = 128
VMEM = pl.BlockSpec(memory_space=pltpu.VMEM)
SMEM = pl.BlockSpec(memory_space=pltpu.SMEM)
HBM = pl.BlockSpec(memory_space=pltpu.HBM)


def rotate(value, axis, by):
    size = lax.axis_size(axis)
    return lax.ppermute(value, axis, [(i, (i + by) % size) for i in range(size)])


def swap_cores(value):
    return lax.ppermute(value, "tp", [(i, i ^ 1) for i in range(lax.axis_size("tp"))])


def ahead(me, by, size):
    return lax.rem(me + jnp.uint32(by % size), jnp.uint32(size))


def swap_groups(value):
    return lax.ppermute(value, "grp", [(i, i ^ 1) for i in range(lax.axis_size("grp"))])


def step_on(value, by):
    return rotate(value, "fs", by)


def ring(shard, half, rest):
    size = lax.axis_size("fs")
    pieces = [shard]
    ups, downs = [half, rest], [half, rest]
    for _ in range(1, size // 2):
        ups = [step_on(v, 1) for v in ups]
        downs = [step_on(v, -1) for v in downs]
        other = swap_groups(jnp.stack([ups[0], downs[0]]))
        pieces += [*ups, *downs, other]
    far = []
    for up, down in zip(ups, downs):
        cut = up.shape[0] // 32 * 16
        far += [step_on(up[:cut], 1), step_on(down[cut:], -1)]
    ours = jnp.concatenate(far[:2])
    return [*pieces, ours, *far[2:], swap_groups(ours)]


def gather_tp(mine):
    back = rotate(mine, "tp", 2)
    front = rotate(mine, "tp", -2)
    far = rotate(mine, "tp", 4)
    same = jnp.stack([mine, front, far, back])
    return same, swap_cores(same)


def scatter_tp(keep, give):
    chips = keep.shape[0]
    here = lax.axis_index("tp").astype(jnp.uint32) // 2
    both = keep.astype(F32) + swap_cores(give).astype(F32)

    def block(d):
        return lax.dynamic_index_in_dim(both, ahead(here, d, chips), 0, keepdims=False).astype(BF16)

    own = lax.dynamic_index_in_dim(both, here, 0, keepdims=False)
    a = rotate(block(1), "tp", 2)
    b = rotate(block(3), "tp", -2)
    c = rotate(block(2), "tp", 4)
    return own + a.astype(F32) + b.astype(F32) + c.astype(F32)


def put(ref, row, parts):
    for (part, copy), rows in parts:
        copy.wait()
        v = part[...]
        if v.shape[0] == 1:
            hi = v.astype(BF16)
            mid = (v - hi.astype(F32)).astype(BF16)
            low = (v - hi.astype(F32) - mid.astype(F32)).astype(BF16)
            line = lax.broadcasted_iota(jnp.int32, (rows, LANES), 0)
            hi, mid, low = (jnp.broadcast_to(t.astype(F32), (rows, LANES)) for t in (hi, mid, low))
            v = jnp.where(line == 0, hi, jnp.where(line == 1, mid, jnp.where(line == 2, low, 0.0)))
        ref[row : row + rows, :] = v.astype(BF16)
        row += rows


def fetch(sources, buffers, sems):
    copies = [pltpu.make_async_copy(a, b, sems.at[k]) for k, (a, b) in enumerate(zip(sources, buffers))]
    for c in copies:
        c.start()
    return list(zip(buffers, copies))


def pack_first_body(place_ref, *refs):
    shard_ref, half_ref, rest_ref, two_ref = refs[8:12]
    left, right, out, out_scale, gate, up, down, down_scale = fetch(refs[:8], refs[12:20], refs[20])
    put(two_ref, 0, [(left, LANES), (right, LANES), (out, out[0].shape[0]), (out_scale, 16)])
    half, down_rows = gate[0].shape[0], down[0].shape[0]
    put(shard_ref, 0, [(gate, half), (up, half), (down, down_rows), (down_scale, 32)])
    half_ref[...] = jnp.where(place_ref[3] == 0, shard_ref[:half], shard_ref[half : 2 * half])
    rest_ref[...] = shard_ref[2 * half :]


def pack_first(where, left, right, out, out_scale, gate, up, down, down_scale):
    half, rest = gate.shape[0], down.shape[0] + 32
    rows = [2 * half + rest, half, rest, 2 * LANES + out.shape[0] + 16]
    sources = [left, right, out, out_scale[None], gate, up, down, down_scale[None]]
    return pl.pallas_call(
        pack_first_body,
        out_shape=[jax.ShapeDtypeStruct((n, LANES), BF16) for n in rows],
        in_specs=[SMEM] + [HBM] * len(sources),
        out_specs=[VMEM] * len(rows),
        scratch_shapes=[pltpu.VMEM(a.shape, F32) for a in sources] + [pltpu.SemaphoreType.DMA((len(sources),))],
        compiler_params=pltpu.CompilerParams(vmem_limit_bytes=8 * 1024 * 1024),
        name="pack_first",
    )(where, *in_hbm(sources))


def pack_second_body(*refs):
    gate, up, down, down_scale = fetch(refs[:4], refs[5:9], refs[9])
    put(refs[4], 0, [(gate, gate[0].shape[0]), (up, up[0].shape[0]), (down, down[0].shape[0]), (down_scale, 16)])


def pack_second(gate, up, down, down_scale):
    rows = gate.shape[0] + up.shape[0] + down.shape[0] + 16
    sources = [gate, up, down, down_scale[None]]
    return pl.pallas_call(
        pack_second_body,
        out_shape=jax.ShapeDtypeStruct((rows, LANES), BF16),
        in_specs=[HBM] * len(sources),
        out_specs=VMEM,
        scratch_shapes=[pltpu.VMEM(a.shape, F32) for a in sources] + [pltpu.SemaphoreType.DMA((len(sources),))],
        compiler_params=pltpu.CompilerParams(vmem_limit_bytes=8 * 1024 * 1024),
        name="pack_second",
    )(*in_hbm(sources))


def nt(a, b):
    return lax.dot_general(a, b, (((1,), (1,)), ((), ())), preferred_element_type=F32)


def nn(a, b):
    return lax.dot_general(a, b, (((1,), (0,)), ((), ())), preferred_element_type=F32)


def chunks_of(n, step=256):
    return [(at, min(step, n - at)) for at in range(0, n, step)]


def normalise(place_ref, same_ref, other_ref, vec_ref, at, raw, xn):
    chips, tokens, width = same_ref.shape
    here, core = place_ref[0], place_ref[1]
    for d in range(chips):
        chip = (here + d) % chips
        raw[2 * chip + core] = same_ref[d]
        raw[2 * chip + 1 - core] = other_ref[d]
    total = jnp.zeros((tokens, 1), F32)
    for j in range(2 * chips):
        v = raw[j].astype(F32)
        total = total + jnp.sum(v * v, axis=1, keepdims=True)
    inverse = lax.rsqrt(total / (2 * chips * width) + EPS)
    for j in range(2 * chips):
        v = raw[j].astype(F32)
        xn[:, j * width : (j + 1) * width] = (v * inverse * vec_ref[:, at + j * width : at + (j + 1) * width]).astype(BF16)


def lanes(ref, row, n, first, count):
    return jnp.concatenate([ref[f, row : row + n, :] for f in range(first, first + count)], axis=1)


def emit(core, hid, w, row, hidden, scale_row, keep_ref, give_ref):
    per = keep_ref.shape[2] // LANES
    for k in range(keep_ref.shape[0]):
        pair = []
        for c in range(2):
            f = (2 * k + c) * per
            s = lanes(w, scale_row, 16, f, per).astype(F32)
            s = jnp.sum(s, axis=0, keepdims=True)
            pair.append((nn(hid, lanes(w, row, hidden, f, per)) * s).astype(BF16))
        keep_ref[k] = jnp.where(core == 0, pair[0], pair[1])
        give_ref[k] = jnp.where(core == 0, pair[1], pair[0])


def piece_copies(place_ref, pieces, w, sems):
    count, rows, _ = w.shape
    me, odd = place_ref[2], place_ref[3]
    half = pieces[1].shape[0]
    ours_at = pl.multiple_of(odd * half, 16)
    theirs_at = pl.multiple_of((1 - odd) * half, 16)
    last = pl.ds(2 * half, rows - 2 * half)
    halves = [(pieces[0].at[pl.ds(0, 2 * half)], w.at[me, pl.ds(0, 2 * half)])]
    rests = [(pieces[0].at[last], w.at[me, last])]
    for step in range(1, count // 2):
        here = pieces[5 * step - 4 : 5 * step + 1]
        for k in range(2):
            f = (me + (count - step if k == 0 else step)) % count
            halves.append((here[2 * k], w.at[f, pl.ds(ours_at, half)]))
            halves.append((here[-1].at[k], w.at[f, pl.ds(theirs_at, half)]))
            rests.append((here[2 * k + 1], w.at[f, last]))
    ours, first, second, theirs = pieces[-4:]
    f = (me + count // 2) % count
    halves += [(ours, w.at[f, pl.ds(ours_at, half)]), (theirs, w.at[f, pl.ds(theirs_at, half)])]
    cut = first.shape[0]
    rests.append((first, w.at[f, pl.ds(2 * half, cut)]))
    rests.append((second, w.at[f, pl.ds(2 * half + cut, second.shape[0])]))
    copies = [pltpu.make_async_copy(a, b, sems.at[k]) for k, (a, b) in enumerate(halves + rests)]
    return copies[: len(halves)], copies[len(halves) :]


def feed_body(*refs, hidden, offsets, parts):
    place_ref, same_ref, other_ref, vec_ref = refs[:4]
    pieces = refs[4 : 4 + parts]
    keep_ref, give_ref, w, raw, xn, hid, sems = refs[4 + parts :]
    gain_at, gate_at, up_at = offsets
    count, rows, _ = w.shape
    chunks = chunks_of(hidden)
    if parts > 1:
        halves, downs = piece_copies(place_ref, pieces, w, sems)
        early = [halves] + [[]] * (len(chunks) - 1)
    else:
        moves = [(row + at, n) for at, n in chunks for row in (0, hidden)] + [(2 * hidden, rows - 2 * hidden)]
        copies = [
            pltpu.make_async_copy(pieces[0].at[:, pl.ds(at, n), :], w.at[:, pl.ds(at, n), :], sems.at[k])
            for k, (at, n) in enumerate(moves)
        ]
        early = [copies[2 * k : 2 * k + 2] for k in range(len(chunks))]
        downs = copies[2 * len(chunks) :]
    for group in [*early, downs]:
        for c in group:
            c.start()
    normalise(place_ref, same_ref, other_ref, vec_ref, gain_at, raw, xn)
    x = xn[...]
    for (at, n), group in zip(chunks, early):
        for c in group:
            c.wait()
        g = nt(x, lanes(w, at, n, 0, count)) * vec_ref[:, gate_at + at : gate_at + at + n]
        u = nt(x, lanes(w, hidden + at, n, 0, count)) * vec_ref[:, up_at + at : up_at + at + n]
        hid[:, at : at + n] = (g / (1.0 + jnp.exp(-g)) * u).astype(BF16)
    for c in downs:
        c.wait()
    emit(place_ref[1], hid[...], w, 2 * hidden, hidden, 3 * hidden, keep_ref, give_ref)


def in_hbm(arrays):
    return [pltpu.with_memory_space_constraint(a, pltpu.HBM) for a in arrays]


def feed(where, same, other, vec, offsets, hidden, pieces, count):
    chips, tokens, width = same.shape
    wide = 2 * chips * width
    rows = pieces[0].shape[-2]
    out = jax.ShapeDtypeStruct(same.shape, BF16)
    return pl.pallas_call(
        functools.partial(feed_body, hidden=hidden, offsets=offsets, parts=len(pieces)),
        out_shape=(out, out),
        in_specs=[SMEM, VMEM, VMEM, VMEM] + [HBM] * len(pieces),
        out_specs=(VMEM, VMEM),
        scratch_shapes=[
            pltpu.VMEM((count, rows, LANES), BF16),
            pltpu.VMEM((2 * chips, tokens, width), BF16),
            pltpu.VMEM((tokens, wide), BF16),
            pltpu.VMEM((tokens, hidden), BF16),
            pltpu.SemaphoreType.DMA((3 * count,)),
        ],
        compiler_params=pltpu.CompilerParams(vmem_limit_bytes=20 * 1024 * 1024),
        cost_estimate=pl.CostEstimate(
            flops=6 * tokens * hidden * wide, bytes_accessed=2 * count * rows * LANES, transcendentals=tokens * hidden
        ),
        name="feed",
    )(where, same, other, vec, *in_hbm(pieces))


def gelu(t):
    return 0.5 * t * (1.0 + jnp.tanh(0.7978845608028654 * (t + 0.044715 * t * t * t)))


def branch_body(place_ref, same_ref, other_ref, vec_ref, w_hbm, left_ref, right_ref, stat_ref, raw, xn, w, sem, *, offsets):
    gain_at, left_at, right_at = offsets
    n = left_ref.shape[1]
    copy = pltpu.make_async_copy(w_hbm.at[:, pl.ds(0, 2 * LANES), :], w, sem)
    copy.start()
    normalise(place_ref, same_ref, other_ref, vec_ref, gain_at, raw, xn)
    copy.wait()
    wide = w.shape[0] * LANES
    sides = [w[:, at : at + LANES, :].reshape(wide, n) for at in (0, LANES)]
    both = nn(xn[...], jnp.concatenate(sides, axis=1))
    left_ref[...] = gelu(both[:, :n] * vec_ref[:, left_at : left_at + n])
    right = gelu(both[:, n:] * vec_ref[:, right_at : right_at + n])
    right_ref[...] = right
    sums = jnp.sum(right, axis=1, keepdims=True)
    squares = jnp.sum(right * right, axis=1, keepdims=True)
    column = lax.broadcasted_iota(jnp.int32, right.shape, 1)
    stat_ref[...] = jnp.where(column == 0, sums, squares).T[: stat_ref.shape[0]]


def branch(where, same, other, vec, offsets, n, w):
    chips, tokens, width = same.shape
    part = jax.ShapeDtypeStruct((tokens, n), F32)
    return pl.pallas_call(
        functools.partial(branch_body, offsets=offsets),
        out_shape=(part, part, jax.ShapeDtypeStruct((8, tokens), F32)),
        in_specs=[SMEM, VMEM, VMEM, VMEM, HBM],
        out_specs=(VMEM, VMEM, VMEM),
        scratch_shapes=[
            pltpu.VMEM((2 * chips, tokens, width), BF16),
            pltpu.VMEM((tokens, 2 * chips * width), BF16),
            pltpu.VMEM((w.shape[0], 2 * LANES, n), BF16),
            pltpu.SemaphoreType.DMA,
        ],
        compiler_params=pltpu.CompilerParams(vmem_limit_bytes=12 * 1024 * 1024),
        cost_estimate=pl.CostEstimate(
            flops=4 * tokens * n * 2 * chips * width, bytes_accessed=8 * n * chips * width, transcendentals=2 * tokens * n
        ),
        name="branch",
    )(where, same, other, vec, pltpu.with_memory_space_constraint(w, pltpu.HBM))


def mix_body(place_ref, left_ref, right_ref, stat_ref, vec_ref, spatial_ref, w_hbm, keep_ref, give_ref, gated, w, sem, *, offsets, channels):
    gain_at, bias_at = offsets
    tokens, n = left_ref.shape
    groups, span, _ = spatial_ref.shape
    each = n // groups
    copy = pltpu.make_async_copy(w_hbm.at[:, pl.ds(2 * LANES, w.shape[1]), :], w, sem)
    copy.start()
    lines = jnp.concatenate([stat_ref[...], jnp.zeros((LANES - stat_ref.shape[0], tokens), F32)]).T
    mean = lines[:, 0:1] / channels
    inverse = lax.rsqrt(lines[:, 1:2] / channels - mean * mean + EPS)
    centred = ((right_ref[...] - mean) * inverse * vec_ref[:, gain_at : gain_at + n]).astype(BF16)
    target = lax.broadcasted_iota(jnp.int32, (span, span), 0)
    source = lax.broadcasted_iota(jnp.int32, (span, span), 1)
    for g in range(groups):
        causal = jnp.where(source <= target, spatial_ref[g].astype(F32), 0.0).astype(BF16)
        bias = jnp.broadcast_to(vec_ref[:, bias_at + g * span : bias_at + (g + 1) * span], (LANES, span)).T[:, 0:1]
        for b in range(tokens // span):
            at, to = b * span, g * each
            mixed = nn(causal, centred[at : at + span, to : to + each]) + bias
            gated[at : at + span, to : to + each] = (left_ref[at : at + span, to : to + each] * mixed).astype(BF16)
    copy.wait()
    emit(place_ref[1], gated[...], w, 0, n, n, keep_ref, give_ref)


def mix(where, left, right, stat, vec, offsets, spatial, w, rows, shape):
    tokens, n = left.shape
    out = jax.ShapeDtypeStruct(shape, BF16)
    return pl.pallas_call(
        functools.partial(mix_body, offsets=offsets, channels=n * 2 * shape[0]),
        out_shape=(out, out),
        in_specs=[SMEM] + [VMEM] * 5 + [HBM],
        out_specs=(VMEM, VMEM),
        scratch_shapes=[
            pltpu.VMEM((tokens, n), BF16),
            pltpu.VMEM((w.shape[0], rows - 2 * LANES, LANES), BF16),
            pltpu.SemaphoreType.DMA,
        ],
        compiler_params=pltpu.CompilerParams(vmem_limit_bytes=12 * 1024 * 1024),
        cost_estimate=pl.CostEstimate(
            flops=4 * tokens * n * shape[0] * shape[2], bytes_accessed=4 * n * shape[0] * shape[2], transcendentals=0
        ),
        name="mix",
    )(where, left, right, stat, vec, spatial, pltpu.with_memory_space_constraint(w, pltpu.HBM))


def sum_tp(stat):
    stat = stat + swap_cores(stat)
    return (stat + rotate(stat, "tp", 4)) + (rotate(stat, "tp", 2) + rotate(stat, "tp", -2))


def in_a_row(vectors):
    padded = [jnp.pad(v, (0, -v.shape[0] % LANES)) for v in vectors]
    starts = [sum(p.shape[0] for p in padded[:k]) for k in range(len(padded))]
    return jnp.concatenate(padded)[None], starts


def layer(
    stream,
    first_gain,
    first_gate,
    first_gate_scale,
    first_up,
    first_up_scale,
    first_down,
    first_down_scale,
    mixer_gain,
    mixer_left,
    mixer_left_scale,
    mixer_right,
    mixer_right_scale,
    channel_gain,
    spatial,
    spatial_bias,
    mixer_out,
    mixer_out_scale,
    second_gain,
    second_gate,
    second_gate_scale,
    second_up,
    second_up_scale,
    second_down,
    second_down_scale,
):
    tp = lax.axis_index("tp").astype(jnp.uint32)
    spots = [tp // 2, tp % 2, lax.axis_index("fs"), lax.axis_index("grp").astype(jnp.uint32) % 2]
    where = jnp.stack([i.astype(jnp.int32) for i in spots])
    hidden = first_gate.shape[1]
    n = mixer_left.shape[1]
    branch_rows = 2 * LANES + n + 16
    shard, half, last, two = pack_first(
        where,
        mixer_left,
        mixer_right,
        mixer_out,
        mixer_out_scale,
        first_gate.T,
        first_up.T,
        first_down,
        first_down_scale,
    )
    one = ring(shard, half, last)
    two = lax.all_gather(two, "fs")
    three = pack_second(second_gate.T, second_up.T, second_down, second_down_scale)
    three = lax.all_gather(three, "fs")
    vec, at = in_a_row(
        [
            first_gain,
            first_gate_scale,
            first_up_scale,
            mixer_gain,
            mixer_left_scale,
            mixer_right_scale,
            channel_gain,
            spatial_bias.reshape(-1),
            second_gain,
            second_gate_scale,
            second_up_scale,
        ]
    )

    rest = stream.T
    same, other = gather_tp(rest)
    keep, give = feed(where, same, other, vec, at[0:3], hidden, one, two.shape[0])
    rest = (rest.astype(F32) + 0.5 * scatter_tp(keep, give)).astype(BF16)

    same, other = gather_tp(rest)
    left, right, stat = branch(where, same, other, vec, at[3:6], n, two)
    keep, give = mix(where, left, right, sum_tp(stat), vec, at[6:8], spatial, two, branch_rows, same.shape)
    rest = (rest.astype(F32) + scatter_tp(keep, give)).astype(BF16)

    same, other = gather_tp(rest)
    keep, give = feed(where, same, other, vec, at[8:11], hidden, [three], two.shape[0])
    return (rest.astype(F32) + 0.5 * scatter_tp(keep, give)).astype(BF16).T


def solution(mesh):
    return jax.shard_map(
        layer,
        mesh=mesh,
        in_specs=(
            P("tp", ("grp", "fs")),
            P(),
            P("fs", "tp"),
            P("tp"),
            P("fs", "tp"),
            P("tp"),
            P("tp", "fs"),
            P("fs"),
            P(),
            P("fs", "tp"),
            P("tp"),
            P("fs", "tp"),
            P("tp"),
            P("tp"),
            P("tp", None, None),
            P("tp", None),
            P("tp", "fs"),
            P("fs"),
            P(),
            P("fs", "tp"),
            P("tp"),
            P("fs", "tp"),
            P("tp"),
            P("tp", "fs"),
            P("fs"),
        ),
        out_specs=P("tp", ("grp", "fs")),
        check_vma=False,
    )
```

```python
import functools

import jax
import jax.numpy as jnp
from jax import lax
from jax.experimental import pallas as pl
from jax.experimental.pallas import tpu as pltpu
from jax.sharding import PartitionSpec as P


EPS = 1e-06
F32 = jnp.float32
BF16 = jnp.bfloat16
LANES = 128
VMEM = pl.BlockSpec(memory_space=pltpu.VMEM)
SMEM = pl.BlockSpec(memory_space=pltpu.SMEM)
HBM = pl.BlockSpec(memory_space=pltpu.HBM)


def rotate(value, axis, by):
    size = lax.axis_size(axis)
    return lax.ppermute(value, axis, [(i, (i + by) % size) for i in range(size)])


def swap_cores(value):
    return lax.ppermute(value, "tp", [(i, i ^ 1) for i in range(lax.axis_size("tp"))])


def ahead(me, by, size):
    return lax.rem(me + jnp.uint32(by % size), jnp.uint32(size))


def swap_groups(value):
    return lax.ppermute(value, "grp", [(i, i ^ 1) for i in range(lax.axis_size("grp"))])


def step_on(value, by):
    return rotate(value, "fs", by)


def ring(shard, half, rest):
    size = lax.axis_size("fs")
    pieces = [shard]
    ups, downs = [half, rest], [half, rest]
    for _ in range(1, size // 2):
        ups = [step_on(v, 1) for v in ups]
        downs = [step_on(v, -1) for v in downs]
        other = swap_groups(jnp.stack([ups[0], downs[0]]))
        pieces += [*ups, *downs, other]
    far = []
    for up, down in zip(ups, downs):
        cut = up.shape[0] // 32 * 16
        far += [step_on(up[:cut], 1), step_on(down[cut:], -1)]
    ours = jnp.concatenate(far[:2])
    other = swap_groups(ours)
    return [*pieces, ours, *far[2:], other]


def gather_tp(mine):
    back = rotate(mine, "tp", 2)
    front = rotate(mine, "tp", -2)
    far = rotate(mine, "tp", 4)
    same = jnp.stack([mine, front, far, back])
    return same, swap_cores(same)


def scatter_tp(keep, give):
    chips = keep.shape[0]
    here = lax.axis_index("tp").astype(jnp.uint32) // 2
    both = keep.astype(F32) + swap_cores(give).astype(F32)

    def block(d):
        return lax.dynamic_index_in_dim(both, ahead(here, d, chips), 0, keepdims=False).astype(BF16)

    own = lax.dynamic_index_in_dim(both, here, 0, keepdims=False)
    a = rotate(block(1), "tp", 2)
    b = rotate(block(3), "tp", -2)
    c = rotate(block(2), "tp", 4)
    return own + a.astype(F32) + b.astype(F32) + c.astype(F32)


def put(ref, row, parts):
    for (part, copy), rows in parts:
        copy.wait()
        v = part[...]
        if v.shape[0] == 1:
            hi = v.astype(BF16)
            mid = (v - hi.astype(F32)).astype(BF16)
            low = (v - hi.astype(F32) - mid.astype(F32)).astype(BF16)
            line = lax.broadcasted_iota(jnp.int32, (rows, LANES), 0)
            hi, mid, low = (jnp.broadcast_to(t.astype(F32), (rows, LANES)) for t in (hi, mid, low))
            v = jnp.where(line == 0, hi, jnp.where(line == 1, mid, jnp.where(line == 2, low, 0.0)))
        ref[row : row + rows, :] = v.astype(BF16)
        row += rows


def fetch(sources, buffers, sems):
    copies = [pltpu.make_async_copy(a, b, sems.at[k]) for k, (a, b) in enumerate(zip(sources, buffers))]
    for c in copies:
        c.start()
    return list(zip(buffers, copies))


def pack_first_body(place_ref, *refs):
    shard_ref, half_ref, rest_ref, two_ref = refs[8:12]
    left, right, out, out_scale, gate, up, down, down_scale = fetch(refs[:8], refs[12:20], refs[20])
    put(two_ref, 0, [(left, LANES), (right, LANES), (out, out[0].shape[0]), (out_scale, 16)])
    half, down_rows = gate[0].shape[0], down[0].shape[0]
    put(shard_ref, 0, [(gate, half), (up, half), (down, down_rows), (down_scale, 16)])
    half_ref[...] = jnp.where(place_ref[3] == 0, shard_ref[:half], shard_ref[half : 2 * half])
    rest_ref[...] = shard_ref[2 * half :]


def pack_first(where, left, right, out, out_scale, gate, up, down, down_scale):
    half, rest = gate.shape[0], down.shape[0] + 16
    rows = [2 * half + rest, half, rest, 2 * LANES + out.shape[0] + 16]
    sources = [left, right, out, out_scale[None], gate, up, down, down_scale[None]]
    return pl.pallas_call(
        pack_first_body,
        out_shape=[jax.ShapeDtypeStruct((n, LANES), BF16) for n in rows],
        in_specs=[SMEM] + [HBM] * len(sources),
        out_specs=[VMEM] * len(rows),
        scratch_shapes=[pltpu.VMEM(a.shape, F32) for a in sources] + [pltpu.SemaphoreType.DMA((len(sources),))],
        compiler_params=pltpu.CompilerParams(vmem_limit_bytes=8 * 1024 * 1024),
        name="pack_first",
    )(where, *in_hbm(sources))


def pack_second_body(*refs):
    gate, up, down, down_scale = fetch(refs[:4], refs[5:9], refs[9])
    put(refs[4], 0, [(gate, gate[0].shape[0]), (up, up[0].shape[0]), (down, down[0].shape[0]), (down_scale, 16)])


def pack_second(gate, up, down, down_scale):
    rows = gate.shape[0] + up.shape[0] + down.shape[0] + 16
    sources = [gate, up, down, down_scale[None]]
    return pl.pallas_call(
        pack_second_body,
        out_shape=jax.ShapeDtypeStruct((rows, LANES), BF16),
        in_specs=[HBM] * len(sources),
        out_specs=VMEM,
        scratch_shapes=[pltpu.VMEM(a.shape, F32) for a in sources] + [pltpu.SemaphoreType.DMA((len(sources),))],
        compiler_params=pltpu.CompilerParams(vmem_limit_bytes=8 * 1024 * 1024),
        name="pack_second",
    )(*in_hbm(sources))


def nt(a, b):
    return lax.dot_general(a, b, (((1,), (1,)), ((), ())), preferred_element_type=F32)


def nn(a, b):
    return lax.dot_general(a, b, (((1,), (0,)), ((), ())), preferred_element_type=F32)


def chunks_of(n, step=256):
    return [(at, min(step, n - at)) for at in range(0, n, step)]


def normalise(place_ref, same_ref, other_ref, vec_ref, at, raw, xn):
    chips, tokens, width = same_ref.shape
    here, core = place_ref[0], place_ref[1]
    for d in range(chips):
        chip = (here + d) % chips
        raw[2 * chip + core] = same_ref[d]
        raw[2 * chip + 1 - core] = other_ref[d]
    total = jnp.zeros((tokens, 1), F32)
    for j in range(2 * chips):
        v = raw[j].astype(F32)
        total = total + jnp.sum(v * v, axis=1, keepdims=True)
    inverse = lax.rsqrt(total / (2 * chips * width) + EPS)
    for j in range(2 * chips):
        v = raw[j].astype(F32)
        xn[:, j * width : (j + 1) * width] = (v * inverse * vec_ref[:, at + j * width : at + (j + 1) * width]).astype(BF16)


def lanes(ref, row, n, first, count):
    return jnp.concatenate([ref[f, row : row + n, :] for f in range(first, first + count)], axis=1)


def emit(core, hid, w, row, hidden, scale_row, keep_ref, give_ref):
    per = keep_ref.shape[2] // LANES
    for k in range(keep_ref.shape[0]):
        pair = []
        for c in range(2):
            f = (2 * k + c) * per
            s = lanes(w, scale_row, 16, f, per).astype(F32)
            s = jnp.sum(s, axis=0, keepdims=True)
            pair.append((nn(hid, lanes(w, row, hidden, f, per)) * s).astype(BF16))
        keep_ref[k] = jnp.where(core == 0, pair[0], pair[1])
        give_ref[k] = jnp.where(core == 0, pair[1], pair[0])


def piece_copies(place_ref, pieces, w, sems):
    count, rows, _ = w.shape
    me, odd = place_ref[2], place_ref[3]
    half = pieces[1].shape[0]
    ours_at = pl.multiple_of(odd * half, 16)
    theirs_at = pl.multiple_of((1 - odd) * half, 16)
    last = pl.ds(2 * half, rows - 2 * half)
    halves = [(pieces[0].at[pl.ds(0, 2 * half)], w.at[me, pl.ds(0, 2 * half)])]
    rests = [(pieces[0].at[last], w.at[me, last])]
    for step in range(1, count // 2):
        here = pieces[5 * step - 4 : 5 * step + 1]
        for k in range(2):
            f = (me + (count - step if k == 0 else step)) % count
            halves.append((here[2 * k], w.at[f, pl.ds(ours_at, half)]))
            halves.append((here[-1].at[k], w.at[f, pl.ds(theirs_at, half)]))
            rests.append((here[2 * k + 1], w.at[f, last]))
    ours, first, second, theirs = pieces[-4:]
    f = (me + count // 2) % count
    halves += [(ours, w.at[f, pl.ds(ours_at, half)]), (theirs, w.at[f, pl.ds(theirs_at, half)])]
    cut = first.shape[0]
    rests.append((first, w.at[f, pl.ds(2 * half, cut)]))
    rests.append((second, w.at[f, pl.ds(2 * half + cut, second.shape[0])]))
    copies = [pltpu.make_async_copy(a, b, sems.at[k]) for k, (a, b) in enumerate(halves + rests)]
    return copies[: len(halves)], copies[len(halves) :]


def feed_body(*refs, hidden, offsets, parts):
    place_ref, same_ref, other_ref, vec_ref = refs[:4]
    pieces = refs[4 : 4 + parts]
    keep_ref, give_ref, w, raw, xn, hid, sems = refs[4 + parts :]
    gain_at, gate_at, up_at = offsets
    count, rows, _ = w.shape
    chunks = chunks_of(hidden)
    if parts > 1:
        halves, downs = piece_copies(place_ref, pieces, w, sems)
        early = [halves] + [[]] * (len(chunks) - 1)
    else:
        moves = [(row + at, n) for at, n in chunks for row in (0, hidden)] + [(2 * hidden, rows - 2 * hidden)]
        copies = [
            pltpu.make_async_copy(pieces[0].at[:, pl.ds(at, n), :], w.at[:, pl.ds(at, n), :], sems.at[k])
            for k, (at, n) in enumerate(moves)
        ]
        early = [copies[2 * k : 2 * k + 2] for k in range(len(chunks))]
        downs = copies[2 * len(chunks) :]
    for group in [*early, downs]:
        for c in group:
            c.start()
    normalise(place_ref, same_ref, other_ref, vec_ref, gain_at, raw, xn)
    x = xn[...]
    for (at, n), group in zip(chunks, early):
        for c in group:
            c.wait()
        g = nt(x, lanes(w, at, n, 0, count)) * vec_ref[:, gate_at + at : gate_at + at + n]
        u = nt(x, lanes(w, hidden + at, n, 0, count)) * vec_ref[:, up_at + at : up_at + at + n]
        hid[:, at : at + n] = (g / (1.0 + jnp.exp(-g)) * u).astype(BF16)
    for c in downs:
        c.wait()
    emit(place_ref[1], hid[...], w, 2 * hidden, hidden, 3 * hidden, keep_ref, give_ref)


def in_hbm(arrays):
    return [pltpu.with_memory_space_constraint(a, pltpu.HBM) for a in arrays]


def feed(where, same, other, vec, offsets, hidden, pieces, count):
    chips, tokens, width = same.shape
    wide = 2 * chips * width
    rows = pieces[0].shape[-2]
    out = jax.ShapeDtypeStruct(same.shape, BF16)
    return pl.pallas_call(
        functools.partial(feed_body, hidden=hidden, offsets=offsets, parts=len(pieces)),
        out_shape=(out, out),
        in_specs=[SMEM, VMEM, VMEM, VMEM] + [HBM] * len(pieces),
        out_specs=(VMEM, VMEM),
        scratch_shapes=[
            pltpu.VMEM((count, rows, LANES), BF16),
            pltpu.VMEM((2 * chips, tokens, width), BF16),
            pltpu.VMEM((tokens, wide), BF16),
            pltpu.VMEM((tokens, hidden), BF16),
            pltpu.SemaphoreType.DMA((3 * count,)),
        ],
        compiler_params=pltpu.CompilerParams(vmem_limit_bytes=20 * 1024 * 1024),
        cost_estimate=pl.CostEstimate(
            flops=6 * tokens * hidden * wide, bytes_accessed=2 * count * rows * LANES, transcendentals=tokens * hidden
        ),
        name="feed",
    )(where, same, other, vec, *in_hbm(pieces))


def gelu(t):
    return 0.5 * t * (1.0 + jnp.tanh(0.7978845608028654 * (t + 0.044715 * t * t * t)))


def branch_body(place_ref, same_ref, other_ref, vec_ref, w_hbm, left_ref, right_ref, stat_ref, raw, xn, w, sem, *, offsets):
    gain_at, left_at, right_at = offsets
    n = left_ref.shape[1]
    copy = pltpu.make_async_copy(w_hbm.at[:, pl.ds(0, 2 * LANES), :], w, sem)
    copy.start()
    normalise(place_ref, same_ref, other_ref, vec_ref, gain_at, raw, xn)
    copy.wait()
    wide = w.shape[0] * LANES
    sides = [w[:, at : at + LANES, :].reshape(wide, n) for at in (0, LANES)]
    both = nn(xn[...], jnp.concatenate(sides, axis=1))
    left_ref[...] = gelu(both[:, :n] * vec_ref[:, left_at : left_at + n])
    right = gelu(both[:, n:] * vec_ref[:, right_at : right_at + n])
    right_ref[...] = right
    sums = jnp.sum(right, axis=1, keepdims=True)
    squares = jnp.sum(right * right, axis=1, keepdims=True)
    column = lax.broadcasted_iota(jnp.int32, right.shape, 1)
    stat_ref[...] = jnp.where(column == 0, sums, squares).T[: stat_ref.shape[0]]


def branch(where, same, other, vec, offsets, n, w):
    chips, tokens, width = same.shape
    part = jax.ShapeDtypeStruct((tokens, n), F32)
    return pl.pallas_call(
        functools.partial(branch_body, offsets=offsets),
        out_shape=(part, part, jax.ShapeDtypeStruct((8, tokens), F32)),
        in_specs=[SMEM, VMEM, VMEM, VMEM, HBM],
        out_specs=(VMEM, VMEM, VMEM),
        scratch_shapes=[
            pltpu.VMEM((2 * chips, tokens, width), BF16),
            pltpu.VMEM((tokens, 2 * chips * width), BF16),
            pltpu.VMEM((w.shape[0], 2 * LANES, n), BF16),
            pltpu.SemaphoreType.DMA,
        ],
        compiler_params=pltpu.CompilerParams(vmem_limit_bytes=12 * 1024 * 1024),
        cost_estimate=pl.CostEstimate(
            flops=4 * tokens * n * 2 * chips * width, bytes_accessed=8 * n * chips * width, transcendentals=2 * tokens * n
        ),
        name="branch",
    )(where, same, other, vec, pltpu.with_memory_space_constraint(w, pltpu.HBM))


def mix_body(place_ref, left_ref, right_ref, stat_ref, vec_ref, spatial_ref, w_hbm, keep_ref, give_ref, gated, w, sem, *, offsets, channels):
    gain_at, bias_at = offsets
    tokens, n = left_ref.shape
    groups, span, _ = spatial_ref.shape
    each = n // groups
    copy = pltpu.make_async_copy(w_hbm.at[:, pl.ds(2 * LANES, w.shape[1]), :], w, sem)
    copy.start()
    lines = jnp.concatenate([stat_ref[...], jnp.zeros((LANES - stat_ref.shape[0], tokens), F32)]).T
    mean = lines[:, 0:1] / channels
    inverse = lax.rsqrt(lines[:, 1:2] / channels - mean * mean + EPS)
    centred = ((right_ref[...] - mean) * inverse * vec_ref[:, gain_at : gain_at + n]).astype(BF16)
    target = lax.broadcasted_iota(jnp.int32, (span, span), 0)
    source = lax.broadcasted_iota(jnp.int32, (span, span), 1)
    for g in range(groups):
        causal = jnp.where(source <= target, spatial_ref[g].astype(F32), 0.0).astype(BF16)
        bias = jnp.broadcast_to(vec_ref[:, bias_at + g * span : bias_at + (g + 1) * span], (LANES, span)).T[:, 0:1]
        for b in range(tokens // span):
            at, to = b * span, g * each
            mixed = nn(causal, centred[at : at + span, to : to + each]) + bias
            gated[at : at + span, to : to + each] = (left_ref[at : at + span, to : to + each] * mixed).astype(BF16)
    copy.wait()
    emit(place_ref[1], gated[...], w, 0, n, n, keep_ref, give_ref)


def mix(where, left, right, stat, vec, offsets, spatial, w, rows, shape):
    tokens, n = left.shape
    out = jax.ShapeDtypeStruct(shape, BF16)
    return pl.pallas_call(
        functools.partial(mix_body, offsets=offsets, channels=n * 2 * shape[0]),
        out_shape=(out, out),
        in_specs=[SMEM] + [VMEM] * 5 + [HBM],
        out_specs=(VMEM, VMEM),
        scratch_shapes=[
            pltpu.VMEM((tokens, n), BF16),
            pltpu.VMEM((w.shape[0], rows - 2 * LANES, LANES), BF16),
            pltpu.SemaphoreType.DMA,
        ],
        compiler_params=pltpu.CompilerParams(vmem_limit_bytes=12 * 1024 * 1024),
        cost_estimate=pl.CostEstimate(
            flops=4 * tokens * n * shape[0] * shape[2], bytes_accessed=4 * n * shape[0] * shape[2], transcendentals=0
        ),
        name="mix",
    )(where, left, right, stat, vec, spatial, pltpu.with_memory_space_constraint(w, pltpu.HBM))


def sum_tp(stat):
    stat = stat + swap_cores(stat)
    return (stat + rotate(stat, "tp", 4)) + (rotate(stat, "tp", 2) + rotate(stat, "tp", -2))


def in_a_row(vectors):
    padded = [jnp.pad(v, (0, -v.shape[0] % LANES)) for v in vectors]
    starts = [sum(p.shape[0] for p in padded[:k]) for k in range(len(padded))]
    return jnp.concatenate(padded)[None], starts


def layer(
    stream,
    first_gain,
    first_gate,
    first_gate_scale,
    first_up,
    first_up_scale,
    first_down,
    first_down_scale,
    mixer_gain,
    mixer_left,
    mixer_left_scale,
    mixer_right,
    mixer_right_scale,
    channel_gain,
    spatial,
    spatial_bias,
    mixer_out,
    mixer_out_scale,
    second_gain,
    second_gate,
    second_gate_scale,
    second_up,
    second_up_scale,
    second_down,
    second_down_scale,
):
    tp = lax.axis_index("tp").astype(jnp.uint32)
    spots = [tp // 2, tp % 2, lax.axis_index("fs"), lax.axis_index("grp").astype(jnp.uint32) % 2]
    where = jnp.stack([i.astype(jnp.int32) for i in spots])
    hidden = first_gate.shape[1]
    n = mixer_left.shape[1]
    branch_rows = 2 * LANES + n + 16
    shard, half, last, two = pack_first(
        where,
        mixer_left,
        mixer_right,
        mixer_out,
        mixer_out_scale,
        first_gate.T,
        first_up.T,
        first_down,
        first_down_scale,
    )
    one = ring(shard, half, last)
    two = lax.all_gather(two, "fs")
    three = pack_second(second_gate.T, second_up.T, second_down, second_down_scale)
    three = lax.all_gather(three, "fs")
    vec, at = in_a_row(
        [
            first_gain,
            first_gate_scale,
            first_up_scale,
            mixer_gain,
            mixer_left_scale,
            mixer_right_scale,
            channel_gain,
            spatial_bias.reshape(-1),
            second_gain,
            second_gate_scale,
            second_up_scale,
        ]
    )

    rest = stream.T
    same, other = gather_tp(rest)
    keep, give = feed(where, same, other, vec, at[0:3], hidden, one, two.shape[0])
    rest = (rest.astype(F32) + 0.5 * scatter_tp(keep, give)).astype(BF16)

    same, other = gather_tp(rest)
    left, right, stat = branch(where, same, other, vec, at[3:6], n, two)
    keep, give = mix(where, left, right, sum_tp(stat), vec, at[6:8], spatial, two, branch_rows, same.shape)
    rest = (rest.astype(F32) + scatter_tp(keep, give)).astype(BF16)

    same, other = gather_tp(rest)
    keep, give = feed(where, same, other, vec, at[8:11], hidden, [three], two.shape[0])
    return (rest.astype(F32) + 0.5 * scatter_tp(keep, give)).astype(BF16).T


def solution(mesh):
    return jax.shard_map(
        layer,
        mesh=mesh,
        in_specs=(
            P("tp", ("grp", "fs")),
            P(),
            P("fs", "tp"),
            P("tp"),
            P("fs", "tp"),
            P("tp"),
            P("tp", "fs"),
            P("fs"),
            P(),
            P("fs", "tp"),
            P("tp"),
            P("fs", "tp"),
            P("tp"),
            P("tp"),
            P("tp", None, None),
            P("tp", None),
            P("tp", "fs"),
            P("fs"),
            P(),
            P("fs", "tp"),
            P("tp"),
            P("fs", "tp"),
            P("tp"),
            P("tp", "fs"),
            P("fs"),
        ),
        out_specs=P("tp", ("grp", "fs")),
        check_vma=False,
    )
```
